32 devices in a mesh: ep: 4 (over y, x), tp: 8 (over z, core).
Axes of the slice: x: 2, y: 2, z: 4, core: 2. Of those that a mesh axis runs over, the one named last changes fastest.
Arguments:
- mix_in: bfloat16 [4096, 2048], P(('ep', 'tp')), may hold values from -6 to 6
- mix_gain: float32 [2048], replicated, may hold values from 0.1 to 1.9
- mix_w_in: bfloat16 [2048, 512], P('tp'), may hold values from -0.125 to 0.125
- pool_mat: bfloat16 [4, 128, 128], replicated, may hold values from -0.5 to 0.5
- pool_scale: float32 [512], replicated, may hold values from 0.1 to 1.9
- mix_w_out: bfloat16 [512, 2048], P(None, 'tp'), may hold values from -0.25 to 0.25
- moe_in: bfloat16 [4096, 2048], P(('ep', 'tp')), may hold values from -6 to 6
- moe_gain: float32 [2048], replicated, may hold values from 0.1 to 1.9
- routes: int32 [4096, 2], P('ep'), may hold values from 0 to 31, all different within a row; in each aligned block of 1024 rows (0 to 1023, 1024 to 2047, ...) at most 128 rows name the same one
- route_score: bfloat16 [4096, 2], P('ep'), may hold values from 0.099609375 to 1
- exp_gate: bfloat16 [32, 2048, 768], P(('ep', 'tp')), may hold values from -0.125 to 0.125
- exp_up: bfloat16 [32, 2048, 768], P(('ep', 'tp')), may hold values from -0.125 to 0.125
- exp_down: bfloat16 [32, 768, 2048], P(('ep', 'tp')), may hold values from -0.21875 to 0.21875
- shared_gate: bfloat16 [768, 2048], P('tp'), may hold values from -0.125 to 0.125
- shared_up: bfloat16 [768, 2048], P('tp'), may hold values from -0.125 to 0.125
- shared_down: bfloat16 [768, 2048], P('tp'), may hold values from -0.21875 to 0.21875
Outputs:
- mixed: bfloat16 [4096, 2048], P(('ep', 'tp'))
- moe_out: bfloat16 [4096, 2048], P(('ep', 'tp'))
The draws below stay inside these ranges and needn't reach their ends.
Inputs may be any that keep to these rules, and one draw needn't show every extreme that they name: `routes`: each row names 2 different experts. Within the rows of one index of ep (aligned blocks of 1024 rows) no expert is named more than 128 times, a bound that some expert reaches in some blocks.
All inputs are finite; a program needn't handle non-finite values.
Results may differ from the reference program's by a relative error of at most 0.012.
Values may be sent and summed in bfloat16 or wider, within the bound.
A program may use at most 128 MiB of HBM per device.

```python
import math
import jax
import jax.numpy as jnp
import numpy as np
from jax import lax

D = 2048
GROUP_CH = 128
POOL_GROUPS = 4
POOL = 512
FF = 768
FF_SH = 768
TOP_K = 2
SEQS_MIX = 1
TOK_MOE = 128
EXPERTS = 32
CAP = 128
TOKENS_MIX = 4096
LEN_MIX = 4096
TOKENS_MOE = 4096
N_EP = 4
N_TP = 8


def shard_levels(own_key, shape, shards, low, high):
    def one(axis_at, blocks):
        draws = jax.random.uniform(jax.random.fold_in(jax.random.fold_in(own_key, 6), axis_at), (blocks,), jnp.float32, low / len(shards), high / len(shards))
        return jnp.repeat(jnp.exp(draws), shape[axis_at] // blocks).reshape((-1,) + (1,) * (len(shape) - axis_at - 1))

    level = one(*shards[0])
    for cut in shards[1:]:
        level = level * one(*cut)
    return level


def deal_out(key, own, number, rows, number_of, top, reach, lean):
    sequence = jax.random.permutation(key, number_of)
    crowded, common = portions_of(number_of, rows * top, reach, lean, True), portions_of(number_of, rows * top, reach, lean, False)
    places = jnp.arange(number_of)

    def named(sizes, turn):
        used = int((sizes > 0).sum())
        fixed = max(1, used // 4)
        shifted = fixed + (places - fixed + turn * (used - fixed)) % max(1, number_of - fixed)
        return jnp.zeros((number_of,), jnp.int32).at[sequence[jnp.where(places < fixed, places, shifted)]].set(jnp.asarray(sizes, jnp.int32))

    sizes = jnp.where(number % 4 == 0, named(crowded, number // 4), named(common, number - number // 4 - 1))
    mixed = jax.random.permutation(jax.random.fold_in(own, 3), number_of)
    donor, taker = mixed[0:number_of // 2 * 2:2], mixed[1:number_of // 2 * 2:2]
    margin = jnp.minimum(sizes[donor] - 1, reach - sizes[taker]) // 2
    margin = jnp.where((donor == sequence[0]) | (taker == sequence[0]) | (sizes[taker] == 0), 0, jnp.maximum(margin, 0))
    shifted = jax.random.randint(jax.random.fold_in(own, 4), (number_of // 2,), 0, 1 << 20) % (margin + 1)
    sizes = sizes.at[donor].add(-shifted).at[taker].add(shifted)
    labels = jnp.searchsorted(jnp.cumsum(sizes), jnp.arange(rows * top), side="right").astype(jnp.int32)
    grid = labels.reshape(top, rows).T
    grid = grid[jax.random.permutation(jax.random.fold_in(own, 1), rows)]
    turn = jax.random.randint(jax.random.fold_in(own, 2), (rows, 1), 0, top)
    return jnp.take_along_axis(grid, (jnp.arange(top)[None, :] + turn) % top, axis=1)


def portions_of(amount, total, most, slope, full):
    weights = [(1 << 20) // math.isqrt(rank ** slope) + 1 for rank in range(1, amount + 1)]
    largest = most if full else min(most, max(-(-total // amount), total * weights[0] // sum(weights)))
    least = 1 if total - largest >= amount - 1 else 0
    given, surplus = [largest] + [least] * (amount - 1), total - largest - least * (amount - 1)
    while surplus > 0:
        candidates = [i for i in range(1, amount) if given[i] < largest] or [i for i in range(1, amount) if given[i] < most]
        mass, budget = sum([weights[i] for i in candidates]), surplus
        for i in candidates:
            addition = min(most - given[i], max(1, budget * weights[i] // mass), surplus)
            given[i] = given[i] + addition
            surplus = surplus - addition
    return np.array(given)


def normal_values(rng, shape, spread, most, split=(), kind=jnp.bfloat16):
    array = spread * jax.random.normal(rng, shape, jnp.float32)
    if split:
        array = array * shard_levels(rng, shape, split, -0.22, 0.18)
    return jnp.clip(array, -most, most).astype(kind)


def setup_inputs(seed: int = 0) -> dict:
    arg_keys = jax.random.split(jax.random.key(seed), 17)
    mix_in = normal_values(arg_keys[0], (TOKENS_MIX, D), 1.0, 6.0, ((0, 32),))
    mix_gain = jnp.clip(1.0 + 0.18 * jax.random.normal(arg_keys[1], (D,), jnp.float32), 0.1, 1.9)
    mix_w_in = normal_values(arg_keys[2], (D, POOL), D ** -0.5, 0.125, ((0, 8),))
    pool_mat = normal_values(arg_keys[3], (POOL_GROUPS, GROUP_CH, GROUP_CH), GROUP_CH ** -0.5, 0.5)
    pool_scale = jnp.clip(1.0 + 0.18 * jax.random.normal(arg_keys[4], (POOL,), jnp.float32), 0.1, 1.9)
    mix_w_out = normal_values(arg_keys[5], (POOL, D), POOL ** -0.5, 0.25, ((1, 8),))
    moe_in = normal_values(arg_keys[6], (TOKENS_MOE, D), 1.0, 6.0, ((0, 32),))
    moe_gain = jnp.clip(1.0 + 0.18 * jax.random.normal(arg_keys[7], (D,), jnp.float32), 0.1, 1.9)
    routes_keys = jax.random.split(jax.random.fold_in(arg_keys[8], 1), TOKENS_MOE // (TOK_MOE * N_TP))
    routes_turns = jax.random.permutation(jax.random.fold_in(arg_keys[8], 3), TOKENS_MOE // (TOK_MOE * N_TP))
    routes = jax.vmap(lambda own, number: deal_out(jax.random.fold_in(arg_keys[8], 2), own, number, TOK_MOE * N_TP, EXPERTS, TOP_K, CAP, 2))(routes_keys, routes_turns).reshape((TOKENS_MOE, TOP_K))
    route_score = jnp.clip(jnp.exp(math.log(1.0) - 2.306499 * jax.random.uniform(arg_keys[9], (TOKENS_MOE, TOP_K), jnp.float32) ** shard_levels(arg_keys[9], (TOKENS_MOE, TOP_K), ((0, 4),), -0.2, 0.2)), 0.099609375, 1.0).astype(jnp.bfloat16)
    exp_gate = normal_values(arg_keys[10], (EXPERTS, D, FF), D ** -0.5, 0.125, ((0, 32),))
    exp_up = normal_values(arg_keys[11], (EXPERTS, D, FF), D ** -0.5, 0.125, ((0, 32),))
    exp_down = normal_values(arg_keys[12], (EXPERTS, FF, D), FF ** -0.5, 0.21875, ((0, 32),))
    shared_gate = normal_values(arg_keys[13], (FF_SH, D), D ** -0.5, 0.125, ((0, 8),))
    shared_up = normal_values(arg_keys[14], (FF_SH, D), D ** -0.5, 0.125, ((0, 8),))
    shared_down = normal_values(arg_keys[15], (FF_SH, D), FF_SH ** -0.5, 0.21875, ((0, 8),))
    return dict(mix_in=mix_in, mix_gain=mix_gain, mix_w_in=mix_w_in, pool_mat=pool_mat, pool_scale=pool_scale, mix_w_out=mix_w_out, moe_in=moe_in, moe_gain=moe_gain, routes=routes, route_score=route_score, exp_gate=exp_gate, exp_up=exp_up, exp_down=exp_down, shared_gate=shared_gate, shared_up=shared_up, shared_down=shared_down)


NORM_EPS = 1e-06
ROUTED_SCALE = 2.5

def rms_rows(values, gain):
    floats = values.astype(jnp.float32)
    scaled = floats * lax.rsqrt(lax.optimization_barrier(jnp.mean(floats * floats, axis=-1, keepdims=True)) + NORM_EPS)
    return (scaled * gain.astype(jnp.float32)).astype(jnp.bfloat16)

def expert_ffn(rows_in, w_gate, w_up, w_down):
    gate_act = jnp.dot(rows_in, w_gate, preferred_element_type=jnp.float32)
    up_act = jnp.dot(rows_in, w_up, preferred_element_type=jnp.float32)
    hidden = (jax.nn.silu(gate_act) * up_act).astype(jnp.bfloat16)
    return jnp.dot(hidden, w_down, preferred_element_type=jnp.float32).astype(jnp.bfloat16)

def mixer_ref(mix_in, mix_gain, mix_w_in, pool_mat, pool_scale, mix_w_out):
    normed = rms_rows(mix_in, mix_gain)
    projected = jnp.dot(normed, mix_w_in, preferred_element_type=jnp.float32).astype(jnp.bfloat16)
    channels = projected.shape[1]
    reach_rows = 2 ** POOL_GROUPS - 1
    floats = projected.astype(jnp.float32).reshape(SEQS_MIX, LEN_MIX, channels)
    padded = jnp.pad(floats, ((0, 0), (reach_rows, 0), (0, 0)))
    position = jnp.arange(LEN_MIX, dtype=jnp.int32)
    pieces = []
    for group in range(POOL_GROUPS):
        window_len = 2 ** (group + 1)
        lower = group * GROUP_CH
        upper = lower + GROUP_CH
        running = jnp.zeros((SEQS_MIX, LEN_MIX, GROUP_CH), jnp.float32)
        for offset in range(window_len):
            running = running + padded[:, reach_rows - offset:reach_rows - offset + LEN_MIX, lower:upper]
        counts = jnp.minimum(position + 1, window_len).astype(jnp.float32)
        pieces.append(running / counts[None, :, None] - floats[:, :, lower:upper])
    pooled = jnp.concatenate(pieces, axis=2).astype(jnp.bfloat16).reshape(-1, POOL_GROUPS, GROUP_CH)
    grouped = jnp.einsum('tgc,gcd->tgd', pooled.astype(jnp.float32), pool_mat.astype(jnp.float32))
    pool_out = (grouped.reshape(-1, channels) * pool_scale).astype(jnp.bfloat16)
    return jnp.dot(pool_out, mix_w_out, preferred_element_type=jnp.float32).astype(jnp.bfloat16)

def experts_ref(moe_in, moe_gain, routes, route_score, exp_gate, exp_up, exp_down, shared_gate, shared_up, shared_down):
    normed = rms_rows(moe_in, moe_gain)
    total_rows, model_width = normed.shape
    block_rows = TOK_MOE * N_TP
    per_block = block_rows * TOP_K
    scores = route_score.astype(jnp.float32)
    weights = scores / lax.optimization_barrier(jnp.sum(scores, axis=1, keepdims=True)) * ROUTED_SCALE
    flat_expert = routes.reshape(N_EP, per_block)
    onehot = (flat_expert[:, :, None] == jnp.arange(EXPERTS, dtype=jnp.int32)[None, None, :]).astype(jnp.int32)
    before = lax.optimization_barrier(jnp.sum((jnp.cumsum(onehot, axis=1) - onehot) * onehot, axis=2))
    block_id = jnp.arange(N_EP, dtype=jnp.int32)[:, None]
    slot_span = N_EP * CAP
    flat_slot = (flat_expert * slot_span + block_id * CAP + before).reshape(-1).astype(jnp.int32)
    token_id = (block_id * block_rows + jnp.arange(per_block, dtype=jnp.int32)[None, :] // TOP_K).reshape(-1)
    table = jnp.full((EXPERTS * slot_span,), total_rows, jnp.int32).at[flat_slot].set(token_id)
    table = table.reshape(EXPERTS, slot_span)
    table_weight = jnp.zeros((EXPERTS * slot_span,), jnp.float32).at[flat_slot].set(weights.reshape(-1))
    table_weight = table_weight.reshape(EXPERTS, slot_span)
    padded_rows = jnp.concatenate([normed, jnp.zeros((1, model_width), jnp.bfloat16)], axis=0)
    gate_act = jnp.dot(normed, shared_gate.T, preferred_element_type=jnp.float32)
    up_act = jnp.dot(normed, shared_up.T, preferred_element_type=jnp.float32)
    shared_hidden = (jax.nn.silu(gate_act) * up_act).astype(jnp.bfloat16)
    shared_out = jnp.dot(shared_hidden, shared_down, preferred_element_type=jnp.float32)

    def column_sum(running, column):

        def one_expert(partial_value, ep_rank):
            expert = ep_rank * N_TP + column
            ids = table[expert]
            rows_in = jnp.take(padded_rows, ids, axis=0)
            outputs = expert_ffn(rows_in, exp_gate[expert], exp_up[expert], exp_down[expert])
            partial_value = partial_value.at[ids].add(outputs.astype(jnp.float32) * table_weight[expert][:, None], mode='drop')
            return (partial_value, None)
        partial_value = jnp.zeros((total_rows, model_width), jnp.float32)
        partial_value, _ = lax.scan(one_expert, partial_value, jnp.arange(N_EP, dtype=jnp.int32))
        return (running + partial_value.astype(jnp.bfloat16).astype(jnp.float32), None)
    running, _ = lax.scan(column_sum, jnp.zeros((total_rows, model_width), jnp.float32), jnp.arange(N_TP, dtype=jnp.int32))
    return (running + shared_out).astype(jnp.bfloat16)

def reference(mix_in, mix_gain, mix_w_in, pool_mat, pool_scale, mix_w_out, moe_in, moe_gain, routes, route_score, exp_gate, exp_up, exp_down, shared_gate, shared_up, shared_down):
    mixed = mixer_ref(mix_in, mix_gain, mix_w_in, pool_mat, pool_scale, mix_w_out)
    moe_out = experts_ref(moe_in, moe_gain, routes, route_score, exp_gate, exp_up, exp_down, shared_gate, shared_up, shared_down)
    return (mixed, moe_out)
```

```python
import functools

import jax
import jax.numpy as jnp
from jax import lax
from jax.experimental import pallas as pl
from jax.experimental.pallas import tpu as pltpu
from jax.sharding import PartitionSpec as P

SEQS_MIX = 1
CORES = 2

NORM_EPS = 1e-06
ROUTED_SCALE = 2.5
MESH = pl.DeviceIdType.MESH
GATHER_CUTS = (4, 4, 4, 4)
RETURN_CUTS = (4, 4, 4, 4)


def rms_rows(values, gain):
    floats = values.astype(jnp.float32)
    scaled = floats * lax.rsqrt(jnp.mean(floats * floats, axis=-1, keepdims=True) + NORM_EPS)
    return (scaled * gain).astype(jnp.bfloat16)


def remote(src, dst, send_sem, recv_sem, device):
    return pltpu.make_async_remote_copy(
        src_ref=src,
        dst_ref=dst,
        send_sem=send_sem,
        recv_sem=recv_sem,
        device_id=device,
        device_id_type=MESH,
    )


def spans_of(width, cuts):
    spans, low = [], 0
    for cut in cuts:
        size = width * cut // sum(cuts)
        spans.append(slice(low, low + size))
        low += size
    return spans


class Place:
    def __init__(self, ep_count, tp_count):
        self.ep_count, self.tp_count = ep_count, tp_count
        self.chips = tp_count // CORES
        self.ep, self.tp = lax.axis_index("ep"), lax.axis_index("tp")
        self.chip, self.core = self.tp // CORES, self.tp % CORES
        self.keys = [(way, d) for d in range(1, self.chips) for way in range(2)]

    def key(self, way, d):
        return self.keys.index((way, d))

    def ahead(self, way):
        return self.chip < self.chips - 1 if way == 0 else self.chip > 0

    def behind(self, way, d):
        return self.chip >= d if way == 0 else self.chip < self.chips - d

    def beyond(self, way, d):
        return self.chip < self.chips - d if way == 0 else self.chip >= d

    def origin(self, way, d):
        return self.chip - d if way == 0 else self.chip + d

    def target(self, way, d):
        return self.chip + d if way == 0 else self.chip - d

    def side(self, way):
        return (self.ep, self.target(way, 1) * CORES + self.core)

    def sibling(self):
        return (self.ep, self.chip * CORES + 1 - self.core)

    def peers(self):
        return [((self.ep + i) % self.ep_count, self.tp) for i in range(1, self.ep_count)]


class LineGather:
    def __init__(self, place, buf, send, recv):
        self.place, self.buf, self.send, self.recv = place, buf, send, recv
        self.count = len(place.keys)

    def block(self, chip, core):
        return self.buf.at[chip, core]

    def push(self, way, d):
        place, n = self.place, self.place.key(way, d)
        block = self.block(place.origin(way, d - 1), place.core)
        return remote(block, block, self.send.at[n], self.recv.at[n], place.side(way))

    def pass_over(self, way, d):
        place, n = self.place, self.count + self.place.key(way, d)
        block = self.block(place.origin(way, d), place.core)
        return remote(block, block, self.send.at[n], self.recv.at[n], place.sibling())

    def own_over(self):
        place, n = self.place, 2 * self.count
        block = self.block(place.chip, place.core)
        return remote(block, block, self.send.at[n], self.recv.at[n], place.sibling())

    def start(self, over=True):
        for way in range(2):
            pl.when(self.place.ahead(way))(lambda way=way: self.push(way, 1).start())
        if over:
            self.own_over().start()

    def step(self, d, onward=True, last=True):
        place = self.place
        for way in range(2):

            def receive(way=way):
                n = place.key(way, d)
                block = self.block(place.origin(way, d), place.core)
                remote(
                    block, block, self.send.at[n], self.recv.at[n], place.sibling()
                ).wait_recv()

            def forward(way=way):
                receive(way)
                if d + 1 < place.chips:
                    self.push(way, d + 1).start()
                self.pass_over(way, d).start()

            def finish(way=way):
                receive(way)
                self.pass_over(way, d).start()

            if onward:
                pl.when(place.behind(way, d) & place.ahead(way))(forward)
            if last:
                pl.when(place.behind(way, d) & jnp.logical_not(place.ahead(way)))(finish)

    def arrive(self):
        place = self.place
        for n, (way, d) in enumerate(place.keys):

            def landed(way=way, d=d, n=n):
                block = self.block(place.origin(way, d), 1 - place.core)
                m = self.count + n
                remote(
                    block, block, self.send.at[m], self.recv.at[m], place.sibling()
                ).wait_recv()

            pl.when(place.behind(way, d))(landed)
        block = self.block(place.chip, 1 - place.core)
        m = 2 * self.count
        remote(block, block, self.send.at[m], self.recv.at[m], place.sibling()).wait_recv()

    def close(self):
        place = self.place
        for way, d in place.keys:
            pl.when(place.behind(way, d - 1) & place.ahead(way))(
                lambda way=way, d=d: self.push(way, d).wait_send()
            )
            pl.when(place.behind(way, d))(
                lambda way=way, d=d: self.pass_over(way, d).wait_send()
            )
        self.own_over().wait_send()


def layer_kernel(
    ep_count, tp_count, seq_len, gather_cuts, return_cuts,
    moe_in, moe_gain, routes, scores, mix_gain, pool_mat, pool_scale,
    shared_gate, shared_up, shared_down, mix_w_in, mix_w_out, mix_in, exp_gate, exp_up, exp_down,
    mixed, moe_out,
    *scratch,
):
    scratch = list(scratch)

    def take(count):
        taken, scratch[:] = scratch[:count], scratch[count:]
        return taken

    gathered, sent_back = len(gather_cuts), len(return_cuts)
    tokens, outgoing, received = take(gathered), take(gathered), take(gathered)
    results, returned = take(sent_back), take(sent_back)
    sums, arrived = take(sent_back), take(sent_back)
    (
        pick, share, w_in, w_out, gate_w, up_w, down_w, gate_sum, up_sum,
        s_gate, s_up, s_down, s_gate_sum, s_up_sum, s_hidden, mix_rows, acc, tail, prior,
        ws, xs, xr, ins, inr, outs, outr, as_, ar, bs, br, cs, cr, hs, hr, ss, sr, rs, rr,
    ) = scratch
    place = Place(ep_count, tp_count)
    chips, chip, core = place.chips, place.chip, place.core
    devices = ep_count * tp_count
    flat = place.ep * tp_count + place.tp
    after, before = (flat + 1) % devices, (flat + devices - 1) % devices
    after = (after // tp_count, after % tp_count)
    before = (before // tp_count, before % tp_count)
    barrier = pltpu.get_barrier_semaphore()

    def greet(device):
        pl.semaphore_signal(barrier, inc=1, device_id=device, device_id_type=MESH)

    near = [place.sibling(), after, before] + place.peers()
    for device in near:
        greet(device)
    for way in range(2):
        pl.when(place.ahead(way))(lambda way=way: greet(place.side(way)))
    stores = (
        (shared_gate, s_gate.at[0]), (shared_up, s_up.at[0]), (shared_down, s_down.at[0]),
        (mix_w_in, w_in.at[chip, core]), (mix_w_out, w_out.at[chip, core]), (mix_in, mix_rows),
        (exp_gate.at[0], gate_w), (exp_up.at[0], up_w), (exp_down.at[0], down_w),
    )
    loads = [pltpu.make_async_copy(src, dst, ws.at[n]) for n, (src, dst) in enumerate(stores)]
    for load in loads:
        load.start()
    rows, width = moe_in.shape
    capacity = outgoing[0].shape[1]
    slots = ep_count * capacity
    block_rows = tp_count * rows
    g_spans, r_spans = spans_of(width, gather_cuts), spans_of(width, return_cuts)
    sent = []

    normed = rms_rows(moe_in[...], moe_gain[...])
    for c, span in enumerate(g_spans):
        tokens[c][pl.ds(chip, 1), pl.ds(core, 1)] = normed[:, span][None, None]
    pl.semaphore_wait(barrier, len(near) + 2 - jnp.where((chip == 0) | (chip == chips - 1), 1, 0))
    gathers = [LineGather(place, tokens[c], xs.at[c], xr.at[c]) for c in range(gathered)]
    gathers[0].start()
    gathers[1].start()

    shared = []
    for n, buf in enumerate((s_gate, s_up, s_down)):
        loads[n].wait()
        copy = remote(buf.at[0], buf.at[1], cs.at[n], cr.at[n], place.sibling())
        copy.start()
        shared.append(copy)

    top_count = routes.shape[0]
    lines = CORES * ep_count
    line = lax.broadcasted_iota(jnp.int32, (lines, block_rows), 0)
    column = chip * CORES + jnp.where(line < ep_count, core, 1 - core)
    names = (line % ep_count) * tp_count + column
    score_rows = scores[...].astype(jnp.float32)
    score_sum = jnp.sum(score_rows, axis=0, keepdims=True)
    named = jnp.zeros((lines, block_rows), jnp.float32)
    weight = jnp.zeros((lines, block_rows), jnp.float32)
    for k in range(top_count):
        hit = routes[k : k + 1, :] == names
        named = named + jnp.where(hit, 1.0, 0.0)
        weight = weight + jnp.where(hit, score_rows[k : k + 1, :] / score_sum * ROUTED_SCALE, 0.0)
    ones = named.astype(jnp.bfloat16)
    earlier = []
    for low in range(0, block_rows, 512):
        source = lax.broadcasted_iota(jnp.int32, (block_rows, 512), 0)
        target = lax.broadcasted_iota(jnp.int32, (block_rows, 512), 1) + low
        strict = jnp.where(source < target, 1.0, 0.0).astype(jnp.bfloat16)
        earlier.append(jnp.dot(ones, strict, preferred_element_type=jnp.float32))
    spot = jnp.where(named > 0.5, jnp.concatenate(earlier, axis=1), -1.0).astype(jnp.int32)
    slot = lax.broadcasted_iota(jnp.int32, (capacity, block_rows), 0)
    for j in range(ep_count):
        here = spot[j : j + 1, :] == slot
        pick[j * capacity : (j + 1) * capacity, :] = jnp.where(here, 1.0, 0.0).astype(jnp.bfloat16)
    slot = lax.broadcasted_iota(jnp.int32, (capacity, rows), 0)
    for b in range(chips):
        low = b * CORES * rows
        even, odd = slice(low, low + rows), slice(low + rows, low + 2 * rows)
        spots = jnp.where(core == 0, spot[:, even], spot[:, odd])
        weights = jnp.where(core == 0, weight[:, even], weight[:, odd])
        for j in range(lines):
            weighed = jnp.where(spots[j : j + 1, :] == slot, weights[j : j + 1, :], 0.0)
            share[b, :, j * capacity : (j + 1) * capacity] = weighed.T.astype(jnp.bfloat16)

    def scatter(source, landing, c, send, recv):
        for i, (peer, column) in enumerate(place.peers()):
            copy = remote(
                source.at[peer], landing.at[place.ep], send.at[c, i], recv.at[c, i],
                (peer, column),
            )
            copy.start()
            sent.append(copy)
        landing[pl.ds(place.ep, 1)] = source[pl.ds(place.ep, 1)]

    def landing_wait(landing, c, i, send, recv):
        peer = (place.ep - i + ep_count) % ep_count
        block = landing.at[peer]
        remote(block, block, send.at[c, i - 1], recv.at[c, i - 1], (peer, place.tp)).wait_recv()

    first = LineGather(place, w_in, ins, inr)
    second = LineGather(place, w_out, outs, outr)
    edge = (chip == 0) | (chip == chips - 1)
    across = (((1,), (1,)), ((), ()))
    for c, span in enumerate(g_spans):
        cut = span.stop - span.start
        for d in range(1, chips):
            gathers[c].step(d)
            if d == 1 and c + 2 < gathered:
                gathers[c + 2].start()
        if c == 0:
            for load in loads[3:5]:
                load.wait()
            for copy in shared:
                copy.wait_recv()
        if c == min(1, gathered - 1):

            @pl.when(edge)
            def _():
                first.start(False)
                second.start(False)

        gathers[c].arrive()
        picked = jnp.dot(
            pick[...], tokens[c][...].reshape(block_rows, cut), preferred_element_type=jnp.float32
        )
        outgoing[c][...] = picked.astype(jnp.bfloat16).reshape(ep_count, capacity, cut)
        scatter(outgoing[c], received[c], c, as_, ar)
        block = tokens[c][:, pl.ds(core, 1)].reshape(chips * rows, cut)
        for acc_ref, part in ((s_gate_sum, s_gate), (s_up_sum, s_up)):
            value = lax.dot_general(
                block, part[:, :, span].reshape(-1, cut), across,
                preferred_element_type=jnp.float32,
            )
            acc_ref[...] = value if c == 0 else acc_ref[...] + value

    @pl.when(jnp.logical_not(edge))
    def _():
        first.start(False)
        second.start(False)

    first.own_over().start()
    second.own_over().start()
    first.step(1, last=False)
    second.step(1, last=False)

    for load in loads[5:]:
        load.wait()
    for c, span in enumerate(g_spans):
        for i in range(1, ep_count):
            landing_wait(received[c], c, i, as_, ar)
        block = received[c][...].reshape(slots, span.stop - span.start)
        for acc_ref, weights in ((gate_sum, gate_w), (up_sum, up_w)):
            value = jnp.dot(block, weights[span, :], preferred_element_type=jnp.float32)
            acc_ref[...] = value if c == 0 else acc_ref[...] + value
    hidden = (jax.nn.silu(gate_sum[...]) * up_sum[...]).astype(jnp.bfloat16)

    def over(c, i):
        peer = (place.ep - i + ep_count) % ep_count
        return remote(
            returned[c].at[0, peer], returned[c].at[1, peer], ss.at[c, i], sr.at[c, i],
            place.sibling(),
        )

    for c, span in enumerate(r_spans):
        value = jnp.dot(hidden, down_w[:, span], preferred_element_type=jnp.float32)
        results[c][...] = value.astype(jnp.bfloat16).reshape(ep_count, capacity, -1)
        scatter(results[c], returned[c].at[0], c, bs, br)
        over(c, 0).start()
    s_hidden[...] = (
        (jax.nn.silu(s_gate_sum[...]) * s_up_sum[...])
        .astype(jnp.bfloat16)
        .reshape(chips, rows, -1)
    )
    for d in range(2, chips):
        first.step(d, last=False)

    def routed(c, b):
        span = r_spans[c]
        cut = span.stop - span.start
        value = jnp.dot(
            share[b], returned[c][...].reshape(CORES * slots, cut),
            preferred_element_type=jnp.float32,
        )
        extra = jnp.dot(
            s_hidden[b], s_down[:, :, span].reshape(-1, cut), preferred_element_type=jnp.float32
        )
        acc[:, :cut] = value + extra

    def landed(c, way, d):
        n = place.key(way, d)
        block = arrived[c].at[n]
        remote(block, block, rs.at[c, n], rr.at[c, n], place.sibling()).wait_recv()
        cut = block.shape[1]
        acc[:, :cut] = acc[:, :cut] + arrived[c][n].astype(jnp.float32)

    def outward(c, way, d):
        n = place.key(way, d)
        return remote(
            sums[c].at[n], arrived[c].at[n], rs.at[c, n], rr.at[c, n], place.side(way)
        )

    def send_sum(c, way, d, joined):
        routed(c, place.target(way, d))
        if joined:
            landed(c, way, d + 1)
        cut = r_spans[c].stop - r_spans[c].start
        sums[c][place.key(way, d)] = acc[:, :cut].astype(jnp.bfloat16)
        outward(c, way, d).start()

    def from_edge(c, d):
        for way in range(2):
            pl.when(place.beyond(way, d) & jnp.logical_not(place.ahead(1 - way)))(
                lambda way=way: send_sum(c, way, d, False)
            )

    def from_middle(c, d):
        for way in range(2):
            pl.when(place.beyond(way, d) & place.ahead(1 - way))(
                lambda way=way: send_sum(c, way, d, True)
            )

    def far_middle(c):
        for d in range(chips - 2, 1, -1):
            from_middle(c, d)

    for c in range(sent_back):
        for i in range(1, ep_count):
            landing_wait(returned[c].at[0], c, i, bs, br)
            over(c, i).start()
        for i in range(ep_count):
            peer = (place.ep - i + ep_count) % ep_count
            block = returned[c].at[1, peer]
            remote(block, block, ss.at[c, i], sr.at[c, i], place.sibling()).wait_recv()
        for d in range(chips - 1, 1, -1):
            from_edge(c, d)
        if c == 0:
            for d in range(2, chips):
                second.step(d, last=False)
        else:
            far_middle(c - 1)
    far_middle(sent_back - 1)
    for c in range(sent_back):
        from_edge(c, 1)
        from_middle(c, 1)

    for d in range(1, chips):
        first.step(d, onward=False)
    first.arrive()
    groups, group_ch = pool_mat.shape[0], pool_mat.shape[1]
    reach = 2**groups
    mix_normed = rms_rows(mix_rows[...], mix_gain[...])
    projected = jnp.dot(
        mix_normed, w_in[...].reshape(width, groups * group_ch), preferred_element_type=jnp.float32
    ).astype(jnp.bfloat16)
    tail[...] = projected[rows - reach :]
    halo = remote(tail, prior, hs, hr, after)
    halo.start()
    for d in range(1, chips):
        second.step(d, onward=False)
    halo.wait()
    first_row = flat * rows
    keep = jnp.where(first_row % seq_len == 0, 0.0, 1.0)
    extended = jnp.concatenate(
        [prior[...].astype(jnp.float32) * keep, projected.astype(jnp.float32)], axis=0
    )
    position = (first_row + lax.broadcasted_iota(jnp.int32, (rows, group_ch), 0)) % seq_len
    pooled_parts = []
    for group in range(groups):
        channels = slice(group * group_ch, (group + 1) * group_ch)
        running = extended[:, channels]
        for level in range(group + 1):
            running = running + pltpu.roll(running, 2**level, 0)
        counts = jnp.minimum(position + 1, 2 ** (group + 1)).astype(jnp.float32)
        pooled = (running[reach:] / counts - extended[reach:, channels]).astype(jnp.bfloat16)
        grouped = jnp.dot(pooled, pool_mat[group], preferred_element_type=jnp.float32)
        pooled_parts.append((grouped * pool_scale[:, channels]).astype(jnp.bfloat16))
    pool_out = jnp.concatenate(pooled_parts, axis=1)
    second.arrive()
    span = w_out.shape[3]
    for column in range(tp_count):
        mixed[:, column * span : (column + 1) * span] = jnp.dot(
            pool_out, w_out[column // CORES, column % CORES], preferred_element_type=jnp.float32
        ).astype(jnp.bfloat16)

    for c, span in enumerate(r_spans):
        routed(c, chip)
        for way in range(2):
            pl.when(place.behind(way, 1))(lambda way=way: landed(c, way, 1))
        moe_out[:, span] = acc[:, : span.stop - span.start].astype(jnp.bfloat16)

    for copy in sent + shared:
        copy.wait_send()
    for c in range(sent_back):
        for i in range(ep_count):
            over(c, i).wait_send()
        for way, d in place.keys:
            pl.when(place.beyond(way, d))(
                lambda way=way, d=d: outward(c, way, d).wait_send()
            )
    for gather in gathers + [first, second]:
        gather.close()


def shards(
    mix_in, mix_gain, mix_w_in, pool_mat, pool_scale, mix_w_out, moe_in, moe_gain, routes,
    route_score, exp_gate, exp_up, exp_down, shared_gate, shared_up, shared_down,
):
    ep_count, tp_count = lax.axis_size("ep"), lax.axis_size("tp")
    rows, width = moe_in.shape
    block_rows, top_count = routes.shape
    capacity = 2 * block_rows * top_count // (ep_count * tp_count)
    slots = ep_count * capacity
    dma = lambda *shape: pltpu.SemaphoreType.DMA(shape)
    bf16, f32 = jnp.bfloat16, jnp.float32

    chips = tp_count // CORES
    messages = 2 * (chips - 1)
    hidden, s_hidden = exp_gate.shape[2], shared_gate.shape[0]
    reach = 2 ** pool_mat.shape[0]
    seq_len = mix_in.shape[0] * ep_count * tp_count // SEQS_MIX
    buffer = lambda *shape: pltpu.VMEM(shape, bf16)
    g_cuts = [s.stop - s.start for s in spans_of(width, GATHER_CUTS)]
    r_cuts = [s.stop - s.start for s in spans_of(width, RETURN_CUTS)]
    gathered, sent_back = len(g_cuts), len(r_cuts)
    mixed, moe_out = pl.pallas_call(
        functools.partial(layer_kernel, ep_count, tp_count, seq_len, GATHER_CUTS, RETURN_CUTS),
        out_shape=[
            jax.ShapeDtypeStruct(mix_in.shape, bf16),
            jax.ShapeDtypeStruct(moe_in.shape, bf16),
        ],
        in_specs=[pl.BlockSpec(memory_space=pltpu.VMEM)] * 7
        + [pl.BlockSpec(memory_space=pl.ANY)] * 9,
        out_specs=[pl.BlockSpec(memory_space=pltpu.VMEM)] * 2,
        scratch_shapes=[buffer(chips, CORES, rows, cut) for cut in g_cuts]
        + [buffer(ep_count, capacity, cut) for cut in g_cuts] * 2
        + [buffer(ep_count, capacity, cut) for cut in r_cuts]
        + [buffer(CORES, ep_count, capacity, cut) for cut in r_cuts]
        + [buffer(messages, rows, cut) for cut in r_cuts] * 2
        + [
            buffer(slots, block_rows),
            buffer(chips, rows, CORES * slots),
            buffer(chips, CORES, *mix_w_in.shape),
            buffer(chips, CORES, *mix_w_out.shape),
            buffer(width, hidden),
            buffer(width, hidden),
            buffer(hidden, width),
            pltpu.VMEM((slots, hidden), f32),
            pltpu.VMEM((slots, hidden), f32),
            buffer(CORES, *shared_gate.shape),
            buffer(CORES, *shared_up.shape),
            buffer(CORES, *shared_down.shape),
            pltpu.VMEM((chips * rows, CORES * s_hidden), f32),
            pltpu.VMEM((chips * rows, CORES * s_hidden), f32),
            buffer(chips, rows, CORES * s_hidden),
            buffer(*mix_in.shape),
            pltpu.VMEM((rows, max(r_cuts)), f32),
            buffer(reach, mix_w_in.shape[1]),
            buffer(reach, mix_w_in.shape[1]),
            dma(9),
            dma(gathered, 2 * messages + 1),
            dma(gathered, 2 * messages + 1),
        ]
        + [dma(2 * messages + 1)] * 4
        + [dma(gathered, ep_count - 1)] * 2
        + [dma(sent_back, ep_count - 1)] * 2
        + [dma(3), dma(3)]
        + [pltpu.SemaphoreType.DMA, pltpu.SemaphoreType.DMA]
        + [dma(sent_back, ep_count)] * 2
        + [dma(sent_back, messages)] * 2,
        compiler_params=pltpu.CompilerParams(
            collective_id=0, has_side_effects=True, vmem_limit_bytes=67043328
        ),
    )(
        moe_in, moe_gain[None, :], routes.T, route_score.T, mix_gain[None, :], pool_mat,
        pool_scale[None, :], shared_gate, shared_up, shared_down, mix_w_in, mix_w_out, mix_in,
        exp_gate, exp_up, exp_down,
    )
    return (mixed, moe_out)


def solution(mesh):
    return jax.shard_map(
        shards,
        mesh=mesh,
        in_specs=(
            P(("ep", "tp"), None),
            P(),
            P("tp", None),
            P(),
            P(),
            P(None, "tp"),
            P(("ep", "tp"), None),
            P(),
            P("ep", None),
            P("ep", None),
            P(("ep", "tp"), None, None),
            P(("ep", "tp"), None, None),
            P(("ep", "tp"), None, None),
            P("tp", None),
            P("tp", None),
            P("tp", None),
        ),
        out_specs=(P(("ep", "tp"), None), P(("ep", "tp"), None)),
        check_vma=False,
    )
```

```python
import functools

import jax
import jax.numpy as jnp
from jax import lax
from jax.experimental import pallas as pl
from jax.experimental.pallas import tpu as pltpu
from jax.sharding import PartitionSpec as P

SEQS_MIX = 1
CORES = 2

NORM_EPS = 1e-06
ROUTED_SCALE = 2.5
MESH = pl.DeviceIdType.MESH
AHEAD = 2
GATHER_CUTS = (1, 1, 1, 1, 1, 1, 1, 1)
RETURN_CUTS = (1, 1, 2, 2, 1, 1)


def rms_rows(values, gain):
    floats = values.astype(jnp.float32)
    scaled = floats * lax.rsqrt(jnp.mean(floats * floats, axis=-1, keepdims=True) + NORM_EPS)
    return (scaled * gain).astype(jnp.bfloat16)


def remote(src, dst, send_sem, recv_sem, device):
    return pltpu.make_async_remote_copy(
        src_ref=src,
        dst_ref=dst,
        send_sem=send_sem,
        recv_sem=recv_sem,
        device_id=device,
        device_id_type=MESH,
    )


def spans_of(width, cuts):
    spans, low = [], 0
    for cut in cuts:
        size = width * cut // sum(cuts)
        spans.append(slice(low, low + size))
        low += size
    return spans


class Place:
    def __init__(self, ep_count, tp_count):
        self.ep_count, self.tp_count = ep_count, tp_count
        self.chips = tp_count // CORES
        self.ep, self.tp = lax.axis_index("ep"), lax.axis_index("tp")
        self.chip, self.core = self.tp // CORES, self.tp % CORES
        self.keys = [(way, d) for d in range(1, self.chips) for way in range(2)]

    def key(self, way, d):
        return self.keys.index((way, d))

    def ahead(self, way):
        return self.chip < self.chips - 1 if way == 0 else self.chip > 0

    def behind(self, way, d):
        return self.chip >= d if way == 0 else self.chip < self.chips - d

    def beyond(self, way, d):
        return self.chip < self.chips - d if way == 0 else self.chip >= d

    def origin(self, way, d):
        return self.chip - d if way == 0 else self.chip + d

    def target(self, way, d):
        return self.chip + d if way == 0 else self.chip - d

    def edge(self, chip):
        return (chip == 0) | (chip == self.chips - 1)

    def side(self, way):
        return (self.ep, self.target(way, 1) * CORES + self.core)

    def sibling(self):
        return (self.ep, self.chip * CORES + 1 - self.core)

    def peers(self):
        return [((self.ep + i) % self.ep_count, self.tp) for i in range(1, self.ep_count)]


class LineGather:
    def __init__(self, place, buf, send, recv):
        self.place, self.buf, self.send, self.recv = place, buf, send, recv
        self.count = len(place.keys)

    def block(self, chip, core):
        return self.buf.at[chip, core]

    def push(self, way, d):
        place, n = self.place, self.place.key(way, d)
        block = self.block(place.origin(way, d - 1), place.core)
        return remote(block, block, self.send.at[n], self.recv.at[n], place.side(way))

    def pass_over(self, way, d):
        place, n = self.place, self.count + self.place.key(way, d)
        block = self.block(place.origin(way, d), place.core)
        return remote(block, block, self.send.at[n], self.recv.at[n], place.sibling())

    def own_over(self):
        place, n = self.place, 2 * self.count
        block = self.block(place.chip, place.core)
        return remote(block, block, self.send.at[n], self.recv.at[n], place.sibling())

    def start(self, over=True):
        for way in range(2):
            pl.when(self.place.ahead(way))(lambda way=way: self.push(way, 1).start())
        if over:
            self.own_over().start()

    def step(self, d, onward=True, last=True, edge=None):
        place = self.place
        for way in range(2):
            outer = place.edge(place.origin(way, d))
            chosen = True if edge is None else outer == edge

            def receive(way=way):
                n = place.key(way, d)
                block = self.block(place.origin(way, d), place.core)
                remote(
                    block, block, self.send.at[n], self.recv.at[n], place.sibling()
                ).wait_recv()

            def forward(way=way):
                receive(way)
                if d + 1 < place.chips:
                    self.push(way, d + 1).start()
                self.pass_over(way, d).start()

            def finish(way=way):
                receive(way)
                self.pass_over(way, d).start()

            if onward:
                pl.when(place.behind(way, d) & place.ahead(way) & chosen)(forward)
            if last:
                pl.when(place.behind(way, d) & jnp.logical_not(place.ahead(way)))(finish)

    def arrive(self):
        place = self.place
        for n, (way, d) in enumerate(place.keys):

            def landed(way=way, d=d, n=n):
                block = self.block(place.origin(way, d), 1 - place.core)
                m = self.count + n
                remote(
                    block, block, self.send.at[m], self.recv.at[m], place.sibling()
                ).wait_recv()

            pl.when(place.behind(way, d))(landed)
        block = self.block(place.chip, 1 - place.core)
        m = 2 * self.count
        remote(block, block, self.send.at[m], self.recv.at[m], place.sibling()).wait_recv()

    def close(self):
        place = self.place
        for way, d in place.keys:
            pl.when(place.behind(way, d - 1) & place.ahead(way))(
                lambda way=way, d=d: self.push(way, d).wait_send()
            )
            pl.when(place.behind(way, d))(
                lambda way=way, d=d: self.pass_over(way, d).wait_send()
            )
        self.own_over().wait_send()


def layer_kernel(
    ep_count, tp_count, seq_len, gather_cuts, return_cuts,
    moe_gain_in, routes_in, scores_in, mix_gain_in, pool_scale_in, moe_in, pool_mat,
    shared_gate, shared_up, shared_down, mix_w_in, mix_w_out, mix_in, exp_gate, exp_up, exp_down,
    mixed, moe_out,
    *scratch,
):
    scratch = list(scratch)

    def take(count):
        taken, scratch[:] = scratch[:count], scratch[count:]
        return taken

    gathered, sent_back = len(gather_cuts), len(return_cuts)
    tokens, outgoing, received = take(gathered), take(gathered), take(gathered)
    results, returned = take(sent_back), take(sent_back)
    sums, arrived = take(sent_back), take(sent_back)
    (
        pick, share, w_in, w_out, gate_w, up_w, down_w, gate_sum, up_sum,
        s_gate, s_up, s_down, s_gate_sum, s_up_sum, s_hidden, moe_rows, mix_rows, mats, acc, own,
        moe_gain, routes, scores, mix_gain, pool_scale,
        ws, xs, xr, ins, inr, outs, outr, as_, ar, bs, br, cs, cr, hs, hr, ss, sr, rs, rr,
    ) = scratch
    place = Place(ep_count, tp_count)
    chips, chip, core = place.chips, place.chip, place.core
    devices = ep_count * tp_count
    flat = place.ep * tp_count + place.tp
    after, before = (flat + 1) % devices, (flat + devices - 1) % devices
    after = (after // tp_count, after % tp_count)
    before = (before // tp_count, before % tp_count)
    barrier = pltpu.get_barrier_semaphore()

    def greet(device):
        pl.semaphore_signal(barrier, inc=1, device_id=device, device_id_type=MESH)

    rows, width = moe_in.shape
    reach = mix_rows.shape[0] - rows
    stores = (
        (moe_in, moe_rows), (moe_gain_in, moe_gain), (routes_in, routes), (scores_in, scores),
        (shared_gate, s_gate.at[0]), (shared_up, s_up.at[0]), (shared_down, s_down.at[0]),
        (mix_w_in, w_in.at[chip, core]), (mix_w_out, w_out.at[chip, core]),
        (mix_in, mix_rows.at[pl.ds(reach, rows)]), (pool_mat, mats),
        (mix_gain_in, mix_gain), (pool_scale_in, pool_scale),
        (exp_gate.at[0], gate_w), (exp_up.at[0], up_w), (exp_down.at[0], down_w),
    )
    loads = [pltpu.make_async_copy(src, dst, ws.at[n]) for n, (src, dst) in enumerate(stores)]
    for load in loads[:4]:
        load.start()
    near = [place.sibling(), after, before] + place.peers()
    for device in near:
        greet(device)
    for way in range(2):
        pl.when(place.ahead(way))(lambda way=way: greet(place.side(way)))
    for load in loads[4:]:
        load.start()
    capacity = outgoing[0].shape[1]
    slots = ep_count * capacity
    block_rows = tp_count * rows
    g_spans, r_spans = spans_of(width, gather_cuts), spans_of(width, return_cuts)
    sent = []

    loads[0].wait()
    loads[1].wait()
    normed = rms_rows(moe_rows[...], moe_gain[...])
    for c, span in enumerate(g_spans):
        tokens[c][pl.ds(chip, 1), pl.ds(core, 1)] = normed[:, span][None, None]
    pl.semaphore_wait(barrier, len(near) + 2 - jnp.where((chip == 0) | (chip == chips - 1), 1, 0))
    gathers = [LineGather(place, tokens[c], xs.at[c], xr.at[c]) for c in range(gathered)]
    for c in range(AHEAD):
        gathers[c].start()

    shared = []
    for n, buf in enumerate((s_gate, s_up, s_down)):
        loads[4 + n].wait()
        copy = remote(buf.at[0], buf.at[1], cs.at[n], cr.at[n], place.sibling())
        copy.start()
        shared.append(copy)

    loads[2].wait()
    loads[3].wait()
    top_count = routes.shape[0]
    lines = CORES * ep_count
    line = lax.broadcasted_iota(jnp.int32, (lines, block_rows), 0)
    column = chip * CORES + jnp.where(line < ep_count, core, 1 - core)
    names = (line % ep_count) * tp_count + column
    score_rows = scores[...].astype(jnp.float32)
    score_sum = jnp.sum(score_rows, axis=0, keepdims=True)
    named = jnp.zeros((lines, block_rows), jnp.float32)
    weight = jnp.zeros((lines, block_rows), jnp.float32)
    for k in range(top_count):
        hit = routes[k : k + 1, :] == names
        named = named + jnp.where(hit, 1.0, 0.0)
        weight = weight + jnp.where(hit, score_rows[k : k + 1, :] / score_sum * ROUTED_SCALE, 0.0)
    ones = named.astype(jnp.bfloat16)
    earlier = []
    for low in range(0, block_rows, 512):
        source = lax.broadcasted_iota(jnp.int32, (block_rows, 512), 0)
        target = lax.broadcasted_iota(jnp.int32, (block_rows, 512), 1) + low
        strict = jnp.where(source < target, 1.0, 0.0).astype(jnp.bfloat16)
        earlier.append(jnp.dot(ones, strict, preferred_element_type=jnp.float32))
    spot = jnp.where(named > 0.5, jnp.concatenate(earlier, axis=1), -1.0).astype(jnp.int32)
    slot = lax.broadcasted_iota(jnp.int32, (capacity, block_rows), 0)
    for j in range(ep_count):
        here = spot[j : j + 1, :] == slot
        pick[j * capacity : (j + 1) * capacity, :] = jnp.where(here, 1.0, 0.0).astype(jnp.bfloat16)
    slot = lax.broadcasted_iota(jnp.int32, (capacity, rows), 0)
    for b in range(chips):
        low = b * CORES * rows
        even, odd = slice(low, low + rows), slice(low + rows, low + 2 * rows)
        spots = jnp.where(core == 0, spot[:, even], spot[:, odd])
        weights = jnp.where(core == 0, weight[:, even], weight[:, odd])
        for j in range(lines):
            weighed = jnp.where(spots[j : j + 1, :] == slot, weights[j : j + 1, :], 0.0)
            share[b, :, j * capacity : (j + 1) * capacity] = weighed.T.astype(jnp.bfloat16)

    def scatter(source, landing, c, send, recv):
        for i, (peer, column) in enumerate(place.peers()):
            copy = remote(
                source.at[peer], landing.at[place.ep], send.at[c, i], recv.at[c, i],
                (peer, column),
            )
            copy.start()
            sent.append(copy)
        landing[pl.ds(place.ep, 1)] = source[pl.ds(place.ep, 1)]

    def landing_wait(landing, c, i, send, recv):
        peer = (place.ep - i + ep_count) % ep_count
        block = landing.at[peer]
        remote(block, block, send.at[c, i - 1], recv.at[c, i - 1], (peer, place.tp)).wait_recv()

    first = LineGather(place, w_in, ins, inr)
    second = LineGather(place, w_out, outs, outr)
    edge = place.edge(chip)
    across = (((1,), (1,)), ((), ()))

    def gate_up(c):
        span = g_spans[c]
        for i in range(1, ep_count):
            landing_wait(received[c], c, i, as_, ar)
        block = received[c][...].reshape(slots, span.stop - span.start)
        for acc_ref, weights in ((gate_sum, gate_w), (up_sum, up_w)):
            value = jnp.dot(block, weights[span, :], preferred_element_type=jnp.float32)
            acc_ref[...] = value if c == 0 else acc_ref[...] + value

    lag = 3
    for turn in range(gathered + chips - 2):
        for d in range(1, chips):
            if 0 <= turn - (d - 1) < gathered:
                gathers[turn - (d - 1)].step(d)
            if d == 1 and turn + AHEAD < gathered:
                gathers[turn + AHEAD].start()
        if turn == 0:
            for load in loads[7:13]:
                load.wait()
            for copy in shared:
                copy.wait_recv()
        if turn == max(0, gathered - 1 - AHEAD):

            @pl.when(edge)
            def _():
                first.start(False)
                second.start(False)

        c = turn - (chips - 2)
        if c < 0:
            continue
        gathers[c].arrive()
        cut = g_spans[c].stop - g_spans[c].start
        picked = jnp.dot(
            pick[...], tokens[c][...].reshape(block_rows, cut), preferred_element_type=jnp.float32
        )
        outgoing[c][...] = picked.astype(jnp.bfloat16).reshape(ep_count, capacity, cut)
        scatter(outgoing[c], received[c], c, as_, ar)
        if c == lag:
            for load in loads[13:]:
                load.wait()
        if c >= lag:
            gate_up(c - lag)

    @pl.when(jnp.logical_not(edge))
    def _():
        first.start(False)
        second.start(False)

    first.step(1, last=False, edge=True)
    second.step(1, last=False, edge=True)
    first.own_over().start()
    second.own_over().start()
    halo = remote(
        mix_rows.at[pl.ds(rows, reach)], mix_rows.at[pl.ds(0, reach)], hs, hr, after
    )
    halo.start()

    for c in range(gathered - lag, gathered - 1):
        gate_up(c)
    for acc_ref, part in ((s_gate_sum, s_gate), (s_up_sum, s_up)):
        value = 0.0
        for c, span in enumerate(g_spans):
            value = value + lax.dot_general(
                tokens[c][:, pl.ds(core, 1)].reshape(chips * rows, -1),
                part[:, :, span].reshape(-1, span.stop - span.start), across,
                preferred_element_type=jnp.float32,
            )
        acc_ref[...] = value
    gate_up(gathered - 1)
    hidden = (jax.nn.silu(gate_sum[...]) * up_sum[...]).astype(jnp.bfloat16)

    def over(c, i):
        peer = (place.ep - i + ep_count) % ep_count
        return remote(
            returned[c].at[0, peer], returned[c].at[1, peer], ss.at[c, i], sr.at[c, i],
            place.sibling(),
        )

    for c, span in enumerate(r_spans):
        value = jnp.dot(hidden, down_w[:, span], preferred_element_type=jnp.float32)
        results[c][...] = value.astype(jnp.bfloat16).reshape(ep_count, capacity, -1)
        scatter(results[c], returned[c].at[0], c, bs, br)
        over(c, 0).start()
    s_hidden[...] = (
        (jax.nn.silu(s_gate_sum[...]) * s_up_sum[...])
        .astype(jnp.bfloat16)
        .reshape(chips, rows, -1)
    )
    first.step(1, last=False, edge=False)

    def routed(c, b):
        span = r_spans[c]
        cut = span.stop - span.start
        value = jnp.dot(
            share[b], returned[c][...].reshape(CORES * slots, cut),
            preferred_element_type=jnp.float32,
        )
        extra = jnp.dot(
            s_hidden[b], s_down[:, :, span].reshape(-1, cut), preferred_element_type=jnp.float32
        )
        acc[:, :cut] = value + extra

    def leaving(way, d):
        return d - 1 if way == 0 else chips - 1 - d

    def reaching(way, d):
        return d - 1 if way == 0 else chips + 1 - d

    def landed(c, way, d, total):
        n = place.key(way, d)
        block = arrived[c].at[reaching(way, d)]
        remote(block, block, rs.at[c, n], rr.at[c, n], place.sibling()).wait_recv()
        total[...] = total[...] + arrived[c][reaching(way, d)].astype(jnp.float32)

    def outward(c, way, d):
        n = place.key(way, d)
        return remote(
            sums[c].at[leaving(way, d)], arrived[c].at[reaching(way, d)], rs.at[c, n],
            rr.at[c, n], place.side(way),
        )

    def from_edge(c, d):
        @pl.when(edge)
        def _():
            up = chip == 0
            pick_way = lambda low, high: jnp.where(up, low, high)
            routed(c, pick_way(place.target(0, d), place.target(1, d)))
            slot = pick_way(leaving(0, d), leaving(1, d))
            cut = r_spans[c].stop - r_spans[c].start
            sums[c][pl.ds(slot, 1)] = acc[:, :cut].astype(jnp.bfloat16)[None]
            n = pick_way(place.key(0, d), place.key(1, d))
            remote(
                sums[c].at[slot], arrived[c].at[pick_way(reaching(0, d), reaching(1, d))],
                rs.at[c, n], rr.at[c, n],
                (place.ep, pick_way(place.target(0, 1), place.target(1, 1)) * CORES + core),
            ).start()

    def from_middle(c, d):
        for way in range(2):

            @pl.when(place.beyond(way, d) & place.ahead(1 - way))
            def _(way=way):
                routed(c, place.target(way, d))
                cut = r_spans[c].stop - r_spans[c].start
                landed(c, way, d + 1, acc.at[:, :cut])
                sums[c][leaving(way, d)] = acc[:, :cut].astype(jnp.bfloat16)
                outward(c, way, d).start()

    def far_middle(c):
        for d in range(chips - 2, 1, -1):
            from_middle(c, d)

    last = sent_back - 1
    for c in range(sent_back):
        for i in range(1, ep_count):
            landing_wait(returned[c].at[0], c, i, bs, br)
            over(c, i).start()
        for i in range(ep_count):
            peer = (place.ep - i + ep_count) % ep_count
            block = returned[c].at[1, peer]
            remote(block, block, ss.at[c, i], sr.at[c, i], place.sibling()).wait_recv()
        for d in range(chips - 1, 0 if c < last - 3 else 1, -1):
            from_edge(c, d)
        if c == 0:
            second.step(1, last=False, edge=False)
        for gather, turn in ((first, 1), (second, 2)):
            if c == min(last, turn):
                for d in range(2, chips):
                    gather.step(d, last=False)
        if c > 0:
            far_middle(c - 1)
        if c > 1:
            from_middle(c - 2, 1)
    far_middle(last)
    for c in range(max(0, last - 3), sent_back):
        from_edge(c, 1)
    for c in range(max(0, last - 1), sent_back):
        from_middle(c, 1)
    for c, span in enumerate(r_spans):
        routed(c, chip)
        own[:, span] = acc[:, : span.stop - span.start]

    for d in range(1, chips):
        first.step(d, onward=False)
    first.arrive()
    halo.wait_recv()
    groups, group_ch = mats.shape[0], mats.shape[1]
    mix_normed = rms_rows(mix_rows[...], mix_gain[...])
    projected = jnp.dot(
        mix_normed, w_in[...].reshape(width, groups * group_ch), preferred_element_type=jnp.float32
    ).astype(jnp.bfloat16)
    first_row = flat * rows
    keep = jnp.where(first_row % seq_len == 0, 0.0, 1.0)
    projected = projected.astype(jnp.float32)
    extended = jnp.concatenate([projected[:reach] * keep, projected[reach:]], axis=0)
    position = (first_row + lax.broadcasted_iota(jnp.int32, (rows, group_ch), 0)) % seq_len
    pooled_parts = []
    for group in range(groups):
        channels = slice(group * group_ch, (group + 1) * group_ch)
        running = extended[:, channels]
        for level in range(group + 1):
            running = running + pltpu.roll(running, 2**level, 0)
        counts = jnp.minimum(position + 1, 2 ** (group + 1)).astype(jnp.float32)
        pooled = (running[reach:] / counts - extended[reach:, channels]).astype(jnp.bfloat16)
        grouped = jnp.dot(pooled, mats[group], preferred_element_type=jnp.float32)
        pooled_parts.append((grouped * pool_scale[:, channels]).astype(jnp.bfloat16))
    pool_out = jnp.concatenate(pooled_parts, axis=1)
    for d in range(1, chips):
        second.step(d, onward=False)
    second.arrive()
    span = w_out.shape[3]
    for column in range(tp_count):
        mixed[:, column * span : (column + 1) * span] = jnp.dot(
            pool_out, w_out[column // CORES, column % CORES], preferred_element_type=jnp.float32
        ).astype(jnp.bfloat16)

    for c, span in enumerate(r_spans):
        for way in range(2):

            def join(way=way):
                landed(c, way, 1, own.at[:, span])

            pl.when(place.behind(way, 1))(join)
        moe_out[:, span] = own[:, span].astype(jnp.bfloat16)

    halo.wait_send()
    for copy in sent + shared:
        copy.wait_send()
    for c in range(sent_back):
        for i in range(ep_count):
            over(c, i).wait_send()
        for way, d in place.keys:
            pl.when(place.beyond(way, d))(
                lambda way=way, d=d: outward(c, way, d).wait_send()
            )
    for gather in gathers + [first, second]:
        gather.close()


def shards(
    mix_in, mix_gain, mix_w_in, pool_mat, pool_scale, mix_w_out, moe_in, moe_gain, routes,
    route_score, exp_gate, exp_up, exp_down, shared_gate, shared_up, shared_down,
):
    ep_count, tp_count = lax.axis_size("ep"), lax.axis_size("tp")
    rows, width = moe_in.shape
    block_rows, top_count = routes.shape
    capacity = 2 * block_rows * top_count // (ep_count * tp_count)
    slots = ep_count * capacity
    dma = lambda *shape: pltpu.SemaphoreType.DMA(shape)
    bf16, f32 = jnp.bfloat16, jnp.float32

    chips = tp_count // CORES
    messages = 2 * (chips - 1)
    hidden, s_hidden = exp_gate.shape[2], shared_gate.shape[0]
    reach = 2 ** pool_mat.shape[0]
    seq_len = mix_in.shape[0] * ep_count * tp_count // SEQS_MIX
    buffer = lambda *shape: pltpu.VMEM(shape, bf16)
    g_cuts = [s.stop - s.start for s in spans_of(width, GATHER_CUTS)]
    r_cuts = [s.stop - s.start for s in spans_of(width, RETURN_CUTS)]
    gathered, sent_back = len(g_cuts), len(r_cuts)
    scratch = (
        [buffer(chips, CORES, rows, cut) for cut in g_cuts]
        + [buffer(ep_count, capacity, cut) for cut in g_cuts] * 2
        + [buffer(ep_count, capacity, cut) for cut in r_cuts]
        + [buffer(CORES, ep_count, capacity, cut) for cut in r_cuts]
        + [buffer(chips - 1, rows, cut) for cut in r_cuts]
        + [buffer(chips + 1, rows, cut) for cut in r_cuts]
        + [
            buffer(slots, block_rows),
            buffer(chips, rows, CORES * slots),
            buffer(chips, CORES, *mix_w_in.shape),
            buffer(chips, CORES, *mix_w_out.shape),
            buffer(width, hidden),
            buffer(width, hidden),
            buffer(hidden, width),
            pltpu.VMEM((slots, hidden), f32),
            pltpu.VMEM((slots, hidden), f32),
            buffer(CORES, *shared_gate.shape),
            buffer(CORES, *shared_up.shape),
            buffer(CORES, *shared_down.shape),
            pltpu.VMEM((chips * rows, CORES * s_hidden), f32),
            pltpu.VMEM((chips * rows, CORES * s_hidden), f32),
            buffer(chips, rows, CORES * s_hidden),
            buffer(*moe_in.shape),
            buffer(mix_in.shape[0] + reach, width),
            buffer(*pool_mat.shape),
            pltpu.VMEM((rows, max(r_cuts)), f32),
            pltpu.VMEM((rows, width), f32),
            pltpu.VMEM((1, width), f32),
            pltpu.VMEM((top_count, block_rows), routes.dtype),
            buffer(top_count, block_rows),
            pltpu.VMEM((1, width), f32),
            pltpu.VMEM((1, pool_scale.shape[0]), f32),
            dma(16),
            dma(gathered, 2 * messages + 1),
            dma(gathered, 2 * messages + 1),
        ]
        + [dma(2 * messages + 1)] * 4
        + [dma(gathered, ep_count - 1)] * 2
        + [dma(sent_back, ep_count - 1)] * 2
        + [dma(3), dma(3)]
        + [pltpu.SemaphoreType.DMA, pltpu.SemaphoreType.DMA]
        + [dma(sent_back, ep_count)] * 2
        + [dma(sent_back, messages)] * 2
    )
    mixed, moe_out = pl.pallas_call(
        functools.partial(layer_kernel, ep_count, tp_count, seq_len, GATHER_CUTS, RETURN_CUTS),
        out_shape=[
            jax.ShapeDtypeStruct(mix_in.shape, bf16),
            jax.ShapeDtypeStruct(moe_in.shape, bf16),
        ],
        in_specs=[pl.BlockSpec(memory_space=pltpu.HBM)] * 16,
        out_specs=[pl.BlockSpec(memory_space=pltpu.VMEM)] * 2,
        scratch_shapes=scratch,
        compiler_params=pltpu.CompilerParams(
            collective_id=0, has_side_effects=True, vmem_limit_bytes=67043328
        ),
    )(
        moe_gain[None, :], routes.T, route_score.T, mix_gain[None, :], pool_scale[None, :],
        moe_in, pool_mat, shared_gate, shared_up, shared_down, mix_w_in, mix_w_out, mix_in,
        exp_gate, exp_up, exp_down,
    )
    return (mixed, moe_out)


def solution(mesh):
    return jax.shard_map(
        shards,
        mesh=mesh,
        in_specs=(
            P(("ep", "tp"), None),
            P(),
            P("tp", None),
            P(),
            P(),
            P(None, "tp"),
            P(("ep", "tp"), None),
            P(),
            P("ep", None),
            P("ep", None),
            P(("ep", "tp"), None, None),
            P(("ep", "tp"), None, None),
            P(("ep", "tp"), None, None),
            P("tp", None),
            P("tp", None),
            P("tp", None),
        ),
        out_specs=(P(("ep", "tp"), None), P(("ep", "tp"), None)),
        check_vma=False,
    )
```

```python
import functools

import jax
import jax.numpy as jnp
from jax import lax
from jax.experimental import pallas as pl
from jax.experimental.pallas import tpu as pltpu
from jax.sharding import PartitionSpec as P

SEQS_MIX = 1
CORES = 2

NORM_EPS = 1e-06
ROUTED_SCALE = 2.5
MESH = pl.DeviceIdType.MESH
AHEAD = 2
LEAD = 5
PROMPT = 2
VMEM_BYTES = 67043328
CHUNKS = 4
GATHER_CUTS = (1, 1, 1, 1, 1, 1, 1, 1)
RETURN_CUTS = (1, 1, 2, 2, 2, 2, 2, 2, 2)


def rms_rows(values, gain):
    floats = values.astype(jnp.float32)
    scaled = floats * lax.rsqrt(jnp.mean(floats * floats, axis=-1, keepdims=True) + NORM_EPS)
    return (scaled * gain).astype(jnp.bfloat16)


def remote(src, dst, send_sem, recv_sem, device):
    return pltpu.make_async_remote_copy(
        src_ref=src,
        dst_ref=dst,
        send_sem=send_sem,
        recv_sem=recv_sem,
        device_id=device,
        device_id_type=MESH,
    )


def spans_of(width, cuts):
    spans, low = [], 0
    for cut in cuts:
        size = width * cut // sum(cuts)
        spans.append(slice(low, low + size))
        low += size
    return spans


class Place:
    def __init__(self, ep_count, tp_count):
        self.ep_count, self.tp_count = ep_count, tp_count
        self.chips = tp_count // CORES
        self.ep, self.tp = lax.axis_index("ep"), lax.axis_index("tp")
        self.chip, self.core = self.tp // CORES, self.tp % CORES
        self.keys = [(way, d) for d in range(1, self.chips) for way in range(2)]

    def key(self, way, d):
        return self.keys.index((way, d))

    def ahead(self, way):
        return self.chip < self.chips - 1 if way == 0 else self.chip > 0

    def behind(self, way, d):
        return self.chip >= d if way == 0 else self.chip < self.chips - d

    def beyond(self, way, d):
        return self.chip < self.chips - d if way == 0 else self.chip >= d

    def origin(self, way, d):
        return self.chip - d if way == 0 else self.chip + d

    def target(self, way, d):
        return self.chip + d if way == 0 else self.chip - d

    def edge(self, chip):
        return (chip == 0) | (chip == self.chips - 1)

    def side(self, way):
        return (self.ep, self.target(way, 1) * CORES + self.core)

    def sibling(self):
        return (self.ep, self.chip * CORES + 1 - self.core)

    def partner(self, i):
        peer, bit = 0, 1
        while bit < self.ep_count:
            peer = peer + (self.ep // bit + i // bit) % 2 * bit
            bit *= 2
        return peer

    def turns(self):
        return range(self.ep_count - 1, 0, -1)


class LineGather:
    def __init__(self, place, buf, send, recv):
        self.place, self.buf, self.send, self.recv = place, buf, send, recv
        self.count = len(place.keys)

    def block(self, chip, core):
        return self.buf.at[chip, core]

    def push(self, way, d):
        place, n = self.place, self.place.key(way, d)
        block = self.block(place.origin(way, d - 1), place.core)
        return remote(block, block, self.send.at[n], self.recv.at[n], place.side(way))

    def pass_over(self, way, d):
        place, n = self.place, self.count + self.place.key(way, d)
        block = self.block(place.origin(way, d), place.core)
        return remote(block, block, self.send.at[n], self.recv.at[n], place.sibling())

    def own_over(self):
        place, n = self.place, 2 * self.count
        block = self.block(place.chip, place.core)
        return remote(block, block, self.send.at[n], self.recv.at[n], place.sibling())

    def start(self, over=True):
        for way in range(2):
            pl.when(self.place.ahead(way))(lambda way=way: self.push(way, 1).start())
        if over:
            self.own_over().start()

    def step(self, d, onward=True, last=True, edge=None):
        place = self.place
        for way in range(2):
            outer = place.edge(place.origin(way, d))
            chosen = True if edge is None else outer == edge

            def receive(way=way):
                n = place.key(way, d)
                block = self.block(place.origin(way, d), place.core)
                remote(
                    block, block, self.send.at[n], self.recv.at[n], place.sibling()
                ).wait_recv()

            def forward(way=way):
                receive(way)
                if d + 1 < place.chips:
                    self.push(way, d + 1).start()
                self.pass_over(way, d).start()

            def finish(way=way):
                receive(way)
                self.pass_over(way, d).start()

            if onward:
                pl.when(place.behind(way, d) & place.ahead(way) & chosen)(forward)
            if last:
                pl.when(place.behind(way, d) & jnp.logical_not(place.ahead(way)))(finish)

    def arrive(self):
        place = self.place
        for n, (way, d) in enumerate(place.keys):

            def landed(way=way, d=d, n=n):
                block = self.block(place.origin(way, d), 1 - place.core)
                m = self.count + n
                remote(
                    block, block, self.send.at[m], self.recv.at[m], place.sibling()
                ).wait_recv()

            pl.when(place.behind(way, d))(landed)
        block = self.block(place.chip, 1 - place.core)
        m = 2 * self.count
        remote(block, block, self.send.at[m], self.recv.at[m], place.sibling()).wait_recv()

    def close(self):
        place = self.place
        for way, d in place.keys:
            pl.when(place.behind(way, d - 1) & place.ahead(way))(
                lambda way=way, d=d: self.push(way, d).wait_send()
            )
            pl.when(place.behind(way, d))(
                lambda way=way, d=d: self.pass_over(way, d).wait_send()
            )
        self.own_over().wait_send()


def layer_kernel(
    ep_count, tp_count, seq_len, gather_cuts, return_cuts,
    moe_gain_in, routes_in, scores_in, mix_gain_in, pool_scale_in, moe_in, pool_mat,
    shared_gate, shared_up, shared_down, mix_w_in, mix_w_out, mix_in, exp_gate, exp_up, exp_down,
    mixed_out, moe_final,
    *scratch,
):
    scratch = list(scratch)

    def take(count):
        taken, scratch[:] = scratch[:count], scratch[count:]
        return taken

    gathered, sent_back = len(gather_cuts), len(return_cuts)
    tokens, outgoing, received = take(gathered), take(gathered), take(gathered)
    results, returned = take(sent_back), take(sent_back)
    sums, arrived = take(sent_back), take(sent_back)
    (
        pick, share, w_in, w_out, gate_w, up_w, down_w, gate_sum, up_sum,
        s_gate, s_up, s_down, s_gate_sum, s_up_sum, s_hidden, moe_rows, mix_rows, mats, acc, own,
        moe_gain, routes, scores, mix_gain, pool_scale, mixed, moe_out, os,
        ws, xs, xr, ins, inr, outs, outr, as_, ar, bs, br, cs, cr, hs, hr, ss, sr, rs, rr,
    ) = scratch
    place = Place(ep_count, tp_count)
    chips, chip, core = place.chips, place.chip, place.core
    devices = ep_count * tp_count
    flat = place.ep * tp_count + place.tp
    after = (flat + 1) % devices
    after = (after // tp_count, after % tp_count)
    barrier = pltpu.get_barrier_semaphore()

    def greet(device):
        pl.semaphore_signal(barrier, inc=1, device_id=device, device_id_type=MESH)

    rows, width = moe_in.shape
    reach = mix_rows.shape[0] - rows
    stores = (
        (moe_in, moe_rows), (moe_gain_in, moe_gain), (routes_in, routes), (scores_in, scores),
        (shared_gate, s_gate.at[0]), (shared_up, s_up.at[0]), (shared_down, s_down.at[0]),
        (mix_w_in, w_in.at[chip, core]), (mix_w_out, w_out.at[chip, core]),
        (mix_in, mix_rows.at[pl.ds(reach, rows)]), (pool_mat, mats),
        (mix_gain_in, mix_gain), (pool_scale_in, pool_scale),
        (exp_gate.at[0], gate_w), (exp_up.at[0], up_w), (exp_down.at[0], down_w),
    )
    loads = [pltpu.make_async_copy(src, dst, ws.at[n]) for n, (src, dst) in enumerate(stores)]
    for load in loads[:4]:
        load.start()
    near = [place.sibling()] + [(place.partner(i), place.tp) for i in place.turns()]
    for device in near:
        greet(device)
    for way in range(2):
        pl.when(place.ahead(way))(lambda way=way: greet(place.side(way)))
    for load in loads[4:]:
        load.start()
    capacity = outgoing[0].shape[1]
    slots = ep_count * capacity
    block_rows = tp_count * rows
    g_spans, r_spans = spans_of(width, gather_cuts), spans_of(width, return_cuts)
    sent = []

    loads[0].wait()
    loads[1].wait()
    normed = rms_rows(moe_rows[...], moe_gain[...])
    for c, span in enumerate(g_spans):
        tokens[c][pl.ds(chip, 1), pl.ds(core, 1)] = normed[:, span][None, None]
    pl.semaphore_wait(barrier, len(near) + 2 - jnp.where((chip == 0) | (chip == chips - 1), 1, 0))
    gathers = [LineGather(place, tokens[c], xs.at[c], xr.at[c]) for c in range(gathered)]
    for c in range(AHEAD):
        gathers[c].start()

    shared = []
    for n, buf in enumerate((s_gate, s_up, s_down)):
        loads[4 + n].wait()
        copy = remote(buf.at[0], buf.at[1], cs.at[n], cr.at[n], place.sibling())
        copy.start()
        shared.append(copy)

    loads[2].wait()
    loads[3].wait()
    top_count = routes.shape[0]
    lines = CORES * ep_count
    line = lax.broadcasted_iota(jnp.int32, (lines, block_rows), 0)
    column = chip * CORES + jnp.where(line < ep_count, core, 1 - core)
    names = (line % ep_count) * tp_count + column
    score_rows = scores[...].astype(jnp.float32)
    score_sum = jnp.sum(score_rows, axis=0, keepdims=True)
    named = jnp.zeros((lines, block_rows), jnp.float32)
    weight = jnp.zeros((lines, block_rows), jnp.float32)
    for k in range(top_count):
        hit = routes[k : k + 1, :] == names
        named = named + jnp.where(hit, 1.0, 0.0)
        weight = weight + jnp.where(hit, score_rows[k : k + 1, :] / score_sum * ROUTED_SCALE, 0.0)
    ones = named.astype(jnp.bfloat16)
    earlier = []
    for low in range(0, block_rows, 512):
        source = lax.broadcasted_iota(jnp.int32, (block_rows, 512), 0)
        target = lax.broadcasted_iota(jnp.int32, (block_rows, 512), 1) + low
        strict = jnp.where(source < target, 1.0, 0.0).astype(jnp.bfloat16)
        earlier.append(jnp.dot(ones, strict, preferred_element_type=jnp.float32))
    spot = jnp.where(named > 0.5, jnp.concatenate(earlier, axis=1), -1.0).astype(jnp.int32)
    slot = lax.broadcasted_iota(jnp.int32, (capacity, block_rows), 0)
    for j in range(ep_count):
        here = spot[j : j + 1, :] == slot
        pick[j * capacity : (j + 1) * capacity, :] = jnp.where(here, 1.0, 0.0).astype(jnp.bfloat16)
    slot = lax.broadcasted_iota(jnp.int32, (capacity, rows), 0)
    for b in range(chips):
        low = b * CORES * rows
        even, odd = slice(low, low + rows), slice(low + rows, low + 2 * rows)
        spots = jnp.where(core == 0, spot[:, even], spot[:, odd])
        weights = jnp.where(core == 0, weight[:, even], weight[:, odd])
        for j in range(lines):
            weighed = jnp.where(spots[j : j + 1, :] == slot, weights[j : j + 1, :], 0.0)
            share[b, :, j * capacity : (j + 1) * capacity] = weighed.T.astype(jnp.bfloat16)

    def scatter(source, landing, c, send, recv):
        for i in place.turns():
            peer = place.partner(i)
            copy = remote(
                source.at[peer], landing.at[place.ep], send.at[c, i - 1], recv.at[c, i - 1],
                (peer, place.tp),
            )
            copy.start()
            sent.append(copy)
        landing[pl.ds(place.ep, 1)] = source[pl.ds(place.ep, 1)]

    def landing_wait(landing, c, i, send, recv):
        peer = place.partner(i)
        block = landing.at[peer]
        remote(block, block, send.at[c, i - 1], recv.at[c, i - 1], (peer, place.tp)).wait_recv()

    first = LineGather(place, w_in, ins, inr)
    second = LineGather(place, w_out, outs, outr)
    edge = place.edge(chip)
    across = (((1,), (1,)), ((), ()))

    def gate_up(c):
        span = g_spans[c]
        for i in place.turns():
            landing_wait(received[c], c, i, as_, ar)
        block = received[c][...].reshape(slots, span.stop - span.start)
        for acc_ref, weights in ((gate_sum, gate_w), (up_sum, up_w)):
            value = jnp.dot(block, weights[span, :], preferred_element_type=jnp.float32)
            acc_ref[...] = value if c == 0 else acc_ref[...] + value

    lag = 3
    for turn in range(gathered + chips - 2):
        for d in range(1, chips):
            if 0 <= turn - (d - 1) < gathered:
                gathers[turn - (d - 1)].step(d)
            if d == 1 and turn + AHEAD < gathered:
                gathers[turn + AHEAD].start()
        if turn == 0:
            for load in loads[7:13]:
                load.wait()
            for copy in shared:
                copy.wait_recv()
        if turn == max(0, gathered - 1 - AHEAD):

            @pl.when(edge)
            def _():
                first.start(False)
                second.start(False)

        c = turn - (chips - 2)
        if c < 0:
            continue
        gathers[c].arrive()
        cut = g_spans[c].stop - g_spans[c].start
        picked = jnp.dot(
            pick[...], tokens[c][...].reshape(block_rows, cut), preferred_element_type=jnp.float32
        )
        outgoing[c][...] = picked.astype(jnp.bfloat16).reshape(ep_count, capacity, cut)
        scatter(outgoing[c], received[c], c, as_, ar)
        if c == lag:
            for load in loads[13:]:
                load.wait()
        if c >= lag:
            gate_up(c - lag)

    @pl.when(jnp.logical_not(edge))
    def _():
        first.start(False)
        second.start(False)

    first.step(1, last=False, edge=True)
    second.step(1, last=False, edge=True)
    first.own_over().start()
    second.own_over().start()
    halo = remote(
        mix_rows.at[pl.ds(rows, reach)], mix_rows.at[pl.ds(0, reach)], hs, hr, after
    )
    halo.start()

    for c in range(gathered - lag, gathered - 1):
        gate_up(c)
    for acc_ref, part in ((s_gate_sum, s_gate), (s_up_sum, s_up)):
        value = 0.0
        for c, span in enumerate(g_spans):
            value = value + lax.dot_general(
                tokens[c][:, pl.ds(core, 1)].reshape(chips * rows, -1),
                part[:, :, span].reshape(-1, span.stop - span.start), across,
                preferred_element_type=jnp.float32,
            )
        acc_ref[...] = value
    gate_up(gathered - 1)
    hidden = (jax.nn.silu(gate_sum[...]) * up_sum[...]).astype(jnp.bfloat16)

    def over(c, i):
        peer = place.partner(i)
        return remote(
            returned[c].at[0, peer], returned[c].at[1, peer], ss.at[c, i], sr.at[c, i],
            place.sibling(),
        )

    def down(c):
        value = jnp.dot(hidden, down_w[:, r_spans[c]], preferred_element_type=jnp.float32)
        results[c][...] = value.astype(jnp.bfloat16).reshape(ep_count, capacity, -1)
        scatter(results[c], returned[c].at[0], c, bs, br)
        over(c, 0).start()

    for c in range(min(LEAD, sent_back)):
        down(c)
    s_hidden[...] = (
        (jax.nn.silu(s_gate_sum[...]) * s_up_sum[...])
        .astype(jnp.bfloat16)
        .reshape(chips, rows, -1)
    )
    first.step(1, last=False, edge=False)

    def routed(c, b):
        span = r_spans[c]
        cut = span.stop - span.start
        value = jnp.dot(
            share[b], returned[c][...].reshape(CORES * slots, cut),
            preferred_element_type=jnp.float32,
        )
        extra = jnp.dot(
            s_hidden[b], s_down[:, :, span].reshape(-1, cut), preferred_element_type=jnp.float32
        )
        acc[:, :cut] = value + extra

    def leaving(way, d):
        return d - 1 if way == 0 else chips - 1 - d

    def reaching(way, d):
        return d - 1 if way == 0 else chips + 1 - d

    def landed(c, way, d, total):
        n = place.key(way, d)
        block = arrived[c].at[reaching(way, d)]
        remote(block, block, rs.at[c, n], rr.at[c, n], place.sibling()).wait_recv()
        total[...] = total[...] + arrived[c][reaching(way, d)].astype(jnp.float32)

    def outward(c, way, d):
        n = place.key(way, d)
        return remote(
            sums[c].at[leaving(way, d)], arrived[c].at[reaching(way, d)], rs.at[c, n],
            rr.at[c, n], place.side(way),
        )

    def from_edge(c, d):
        @pl.when(edge)
        def _():
            up = chip == 0
            pick_way = lambda low, high: jnp.where(up, low, high)
            routed(c, pick_way(place.target(0, d), place.target(1, d)))
            slot = pick_way(leaving(0, d), leaving(1, d))
            cut = r_spans[c].stop - r_spans[c].start
            sums[c][pl.ds(slot, 1)] = acc[:, :cut].astype(jnp.bfloat16)[None]
            n = pick_way(place.key(0, d), place.key(1, d))
            remote(
                sums[c].at[slot], arrived[c].at[pick_way(reaching(0, d), reaching(1, d))],
                rs.at[c, n], rr.at[c, n],
                (place.ep, pick_way(place.target(0, 1), place.target(1, 1)) * CORES + core),
            ).start()

    def from_middle(c, d):
        for way in range(2):

            @pl.when(place.beyond(way, d) & place.ahead(1 - way))
            def _(way=way):
                routed(c, place.target(way, d))
                cut = r_spans[c].stop - r_spans[c].start
                landed(c, way, d + 1, acc.at[:, :cut])
                sums[c][leaving(way, d)] = acc[:, :cut].astype(jnp.bfloat16)
                outward(c, way, d).start()

    def far_middle(c):
        for d in range(chips - 2, 1, -1):
            from_middle(c, d)

    last = sent_back - 1
    for c in range(sent_back):
        if c > 0 and c + LEAD - 1 < sent_back:
            down(c + LEAD - 1)
        for i in place.turns():
            landing_wait(returned[c].at[0], c, i, bs, br)
            over(c, i).start()
        for i in range(ep_count):
            peer = place.partner(i)
            block = returned[c].at[1, peer]
            remote(block, block, ss.at[c, i], sr.at[c, i], place.sibling()).wait_recv()
        for d in range(chips - 1, 0 if c < PROMPT else 1, -1):
            from_edge(c, d)
        if c == 0:
            second.step(1, last=False, edge=False)
        for gather, turn in ((first, 1), (second, 2)):
            if c == min(last, turn):
                for d in range(2, chips):
                    gather.step(d, last=False)
        if c > 0:
            far_middle(c - 1)
        if c > 1:
            from_middle(c - 2, 1)
    far_middle(last)
    for c in range(PROMPT, sent_back):
        from_edge(c, 1)
    for c in range(max(0, last - 1), sent_back):
        from_middle(c, 1)
    for c, span in enumerate(r_spans):
        routed(c, chip)
        own[:, span] = acc[:, : span.stop - span.start]

    for d in range(1, chips):
        first.step(d, onward=False)
    first.arrive()
    halo.wait_recv()
    groups, group_ch = mats.shape[0], mats.shape[1]
    mix_normed = rms_rows(mix_rows[...], mix_gain[...])
    projected = jnp.dot(
        mix_normed, w_in[...].reshape(width, groups * group_ch), preferred_element_type=jnp.float32
    ).astype(jnp.bfloat16)
    first_row = flat * rows
    keep = jnp.where(first_row % seq_len == 0, 0.0, 1.0)
    projected = projected.astype(jnp.float32)
    extended = jnp.concatenate([projected[:reach] * keep, projected[reach:]], axis=0)
    position = (first_row + lax.broadcasted_iota(jnp.int32, (rows, group_ch), 0)) % seq_len
    pooled_parts = []
    for group in range(groups):
        channels = slice(group * group_ch, (group + 1) * group_ch)
        running = extended[:, channels]
        for level in range(group + 1):
            running = running + pltpu.roll(running, 2**level, 0)
        counts = jnp.minimum(position + 1, 2 ** (group + 1)).astype(jnp.float32)
        pooled = (running[reach:] / counts - extended[reach:, channels]).astype(jnp.bfloat16)
        grouped = jnp.dot(pooled, mats[group], preferred_element_type=jnp.float32)
        pooled_parts.append((grouped * pool_scale[:, channels]).astype(jnp.bfloat16))
    pool_out = jnp.concatenate(pooled_parts, axis=1)
    for d in range(1, chips):
        second.step(d, onward=False)
    second.arrive()
    span = w_out.shape[3]
    for column in range(tp_count):
        mixed[:, column * span : (column + 1) * span] = jnp.dot(
            pool_out, w_out[column // CORES, column % CORES], preferred_element_type=jnp.float32
        ).astype(jnp.bfloat16)

    outs = [pltpu.make_async_copy(mixed, mixed_out, os.at[sent_back])]
    outs[0].start()
    for c, span in enumerate(r_spans):
        for way in range(2):

            def join(way=way):
                landed(c, way, 1, own.at[:, span])

            pl.when(place.behind(way, 1))(join)
        moe_out[:, span] = own[:, span].astype(jnp.bfloat16)
        out = pltpu.make_async_copy(moe_out.at[:, span], moe_final.at[:, span], os.at[c])
        out.start()
        outs.append(out)

    halo.wait_send()
    for out in outs:
        out.wait()
    for copy in sent + shared:
        copy.wait_send()
    for c in range(sent_back):
        for i in range(ep_count):
            over(c, i).wait_send()
        for way, d in place.keys:
            pl.when(place.beyond(way, d))(
                lambda way=way, d=d: outward(c, way, d).wait_send()
            )
    for gather in gathers + [first, second]:
        gather.close()


def settle_kernel(mixed, moe, mixed_out, moe_out, held, arrive, leave):
    rows = mixed.shape[0] // CHUNKS
    inward, outward = [], []
    for n, (src, dst) in enumerate(((mixed, mixed_out), (moe, moe_out))):
        for k in range(CHUNKS):
            span = pl.ds(k * rows, rows)
            block = held.at[n, span]
            inward.append(pltpu.make_async_copy(src.at[span], block, arrive.at[n, k]))
            outward.append(pltpu.make_async_copy(block, dst.at[span], leave.at[n, k]))
    for copy in inward:
        copy.start()
    for n, copy in enumerate(inward):
        copy.wait()
        outward[n].start()
    for copy in outward:
        copy.wait()


def shards(
    mix_in, mix_gain, mix_w_in, pool_mat, pool_scale, mix_w_out, moe_in, moe_gain, routes,
    route_score, exp_gate, exp_up, exp_down, shared_gate, shared_up, shared_down,
):
    ep_count, tp_count = lax.axis_size("ep"), lax.axis_size("tp")
    rows, width = moe_in.shape
    block_rows, top_count = routes.shape
    capacity = 2 * block_rows * top_count // (ep_count * tp_count)
    slots = ep_count * capacity
    dma = lambda *shape: pltpu.SemaphoreType.DMA(shape)
    bf16, f32 = jnp.bfloat16, jnp.float32

    chips = tp_count // CORES
    messages = 2 * (chips - 1)
    hidden, s_hidden = exp_gate.shape[2], shared_gate.shape[0]
    reach = 2 ** pool_mat.shape[0]
    seq_len = mix_in.shape[0] * ep_count * tp_count // SEQS_MIX
    buffer = lambda *shape: pltpu.VMEM(shape, bf16)
    g_cuts = [s.stop - s.start for s in spans_of(width, GATHER_CUTS)]
    r_cuts = [s.stop - s.start for s in spans_of(width, RETURN_CUTS)]
    gathered, sent_back = len(g_cuts), len(r_cuts)
    scratch = (
        [buffer(chips, CORES, rows, cut) for cut in g_cuts]
        + [buffer(ep_count, capacity, cut) for cut in g_cuts] * 2
        + [buffer(ep_count, capacity, cut) for cut in r_cuts]
        + [buffer(CORES, ep_count, capacity, cut) for cut in r_cuts]
        + [buffer(chips - 1, rows, cut) for cut in r_cuts]
        + [buffer(chips + 1, rows, cut) for cut in r_cuts]
        + [
            buffer(slots, block_rows),
            buffer(chips, rows, CORES * slots),
            buffer(chips, CORES, *mix_w_in.shape),
            buffer(chips, CORES, *mix_w_out.shape),
            buffer(width, hidden),
            buffer(width, hidden),
            buffer(hidden, width),
            pltpu.VMEM((slots, hidden), f32),
            pltpu.VMEM((slots, hidden), f32),
            buffer(CORES, *shared_gate.shape),
            buffer(CORES, *shared_up.shape),
            buffer(CORES, *shared_down.shape),
            pltpu.VMEM((chips * rows, CORES * s_hidden), f32),
            pltpu.VMEM((chips * rows, CORES * s_hidden), f32),
            buffer(chips, rows, CORES * s_hidden),
            buffer(*moe_in.shape),
            buffer(mix_in.shape[0] + reach, width),
            buffer(*pool_mat.shape),
            pltpu.VMEM((rows, max(r_cuts)), f32),
            pltpu.VMEM((rows, width), f32),
            pltpu.VMEM((1, width), f32),
            pltpu.VMEM((top_count, block_rows), routes.dtype),
            buffer(top_count, block_rows),
            pltpu.VMEM((1, width), f32),
            pltpu.VMEM((1, pool_scale.shape[0]), f32),
            buffer(*mix_in.shape),
            buffer(*moe_in.shape),
            dma(1 + sent_back),
            dma(16),
            dma(gathered, 2 * messages + 1),
            dma(gathered, 2 * messages + 1),
        ]
        + [dma(2 * messages + 1)] * 4
        + [dma(gathered, ep_count - 1)] * 2
        + [dma(sent_back, ep_count - 1)] * 2
        + [dma(3), dma(3)]
        + [pltpu.SemaphoreType.DMA, pltpu.SemaphoreType.DMA]
        + [dma(sent_back, ep_count)] * 2
        + [dma(sent_back, messages)] * 2
    )
    mixed, moe_out = pl.pallas_call(
        functools.partial(layer_kernel, ep_count, tp_count, seq_len, GATHER_CUTS, RETURN_CUTS),
        out_shape=[
            jax.ShapeDtypeStruct(mix_in.shape, bf16),
            jax.ShapeDtypeStruct(moe_in.shape, bf16),
        ],
        in_specs=[pl.BlockSpec(memory_space=pltpu.HBM)] * 16,
        out_specs=[pl.BlockSpec(memory_space=pltpu.HBM)] * 2,
        scratch_shapes=scratch,
        compiler_params=pltpu.CompilerParams(
            collective_id=0, has_side_effects=True, vmem_limit_bytes=VMEM_BYTES
        ),
    )(
        moe_gain[None, :], routes.T, route_score.T, mix_gain[None, :], pool_scale[None, :],
        moe_in, pool_mat, shared_gate, shared_up, shared_down, mix_w_in, mix_w_out, mix_in,
        exp_gate, exp_up, exp_down,
    )
    return pl.pallas_call(
        settle_kernel,
        out_shape=[
            jax.ShapeDtypeStruct(mix_in.shape, bf16),
            jax.ShapeDtypeStruct(moe_in.shape, bf16),
        ],
        in_specs=[pl.BlockSpec(memory_space=pltpu.HBM)] * 2,
        out_specs=[pl.BlockSpec(memory_space=pltpu.HBM)] * 2,
        scratch_shapes=[buffer(2, *mix_in.shape), dma(2, CHUNKS), dma(2, CHUNKS)],
        compiler_params=pltpu.CompilerParams(vmem_limit_bytes=VMEM_BYTES),
    )(mixed, moe_out)


def solution(mesh):
    return jax.shard_map(
        shards,
        mesh=mesh,
        in_specs=(
            P(("ep", "tp"), None),
            P(),
            P("tp", None),
            P(),
            P(),
            P(None, "tp"),
            P(("ep", "tp"), None),
            P(),
            P("ep", None),
            P("ep", None),
            P(("ep", "tp"), None, None),
            P(("ep", "tp"), None, None),
            P(("ep", "tp"), None, None),
            P("tp", None),
            P("tp", None),
            P("tp", None),
        ),
        out_specs=(P(("ep", "tp"), None), P(("ep", "tp"), None)),
        check_vma=False,
    )
```

```python
import functools

import jax
import jax.numpy as jnp
from jax import lax
from jax.experimental import pallas as pl
from jax.experimental.pallas import tpu as pltpu
from jax.sharding import PartitionSpec as P

SEQS_MIX = 1
CORES = 2

NORM_EPS = 1e-06
ROUTED_SCALE = 2.5
MESH = pl.DeviceIdType.MESH
AHEAD = 2
LEAD = 5
PROMPT = 2
VMEM_BYTES = 67043328
CHUNKS = 4
GATHER_CUTS = (1, 2, 2, 2, 2, 2, 2, 2, 1)
RETURN_CUTS = (1, 1, 2, 2, 2, 2, 2, 2, 2)


def rms_rows(values, gain):
    floats = values.astype(jnp.float32)
    scaled = floats * lax.rsqrt(jnp.mean(floats * floats, axis=-1, keepdims=True) + NORM_EPS)
    return (scaled * gain).astype(jnp.bfloat16)


def remote(src, dst, send_sem, recv_sem, device):
    return pltpu.make_async_remote_copy(
        src_ref=src,
        dst_ref=dst,
        send_sem=send_sem,
        recv_sem=recv_sem,
        device_id=device,
        device_id_type=MESH,
    )


def spans_of(width, cuts):
    spans, low = [], 0
    for cut in cuts:
        size = width * cut // sum(cuts)
        spans.append(slice(low, low + size))
        low += size
    return spans


class Place:
    def __init__(self, ep_count, tp_count):
        self.ep_count, self.tp_count = ep_count, tp_count
        self.chips = tp_count // CORES
        self.ep, self.tp = lax.axis_index("ep"), lax.axis_index("tp")
        self.chip, self.core = self.tp // CORES, self.tp % CORES
        self.keys = [(way, d) for d in range(1, self.chips) for way in range(2)]

    def key(self, way, d):
        return self.keys.index((way, d))

    def ahead(self, way):
        return self.chip < self.chips - 1 if way == 0 else self.chip > 0

    def behind(self, way, d):
        return self.chip >= d if way == 0 else self.chip < self.chips - d

    def beyond(self, way, d):
        return self.chip < self.chips - d if way == 0 else self.chip >= d

    def origin(self, way, d):
        return self.chip - d if way == 0 else self.chip + d

    def target(self, way, d):
        return self.chip + d if way == 0 else self.chip - d

    def edge(self, chip):
        return (chip == 0) | (chip == self.chips - 1)

    def side(self, way):
        return (self.ep, self.target(way, 1) * CORES + self.core)

    def sibling(self):
        return (self.ep, self.chip * CORES + 1 - self.core)

    def partner(self, i):
        peer, bit = 0, 1
        while bit < self.ep_count:
            peer = peer + (self.ep // bit + i // bit) % 2 * bit
            bit *= 2
        return peer

    def turns(self):
        return range(self.ep_count - 1, 0, -1)


class LineGather:
    def __init__(self, place, buf, send, recv):
        self.place, self.buf, self.send, self.recv = place, buf, send, recv
        self.count = len(place.keys)

    def block(self, chip, core):
        return self.buf.at[chip, core]

    def push(self, way, d):
        place, n = self.place, self.place.key(way, d)
        block = self.block(place.origin(way, d - 1), place.core)
        return remote(block, block, self.send.at[n], self.recv.at[n], place.side(way))

    def pass_over(self, way, d):
        place, n = self.place, self.count + self.place.key(way, d)
        block = self.block(place.origin(way, d), place.core)
        return remote(block, block, self.send.at[n], self.recv.at[n], place.sibling())

    def own_over(self):
        place, n = self.place, 2 * self.count
        block = self.block(place.chip, place.core)
        return remote(block, block, self.send.at[n], self.recv.at[n], place.sibling())

    def start(self, over=True):
        for way in range(2):
            pl.when(self.place.ahead(way))(lambda way=way: self.push(way, 1).start())
        if over:
            self.own_over().start()

    def step(self, d, onward=True, last=True, edge=None):
        place = self.place
        for way in range(2):
            outer = place.edge(place.origin(way, d))
            chosen = True if edge is None else outer == edge

            def receive(way=way):
                n = place.key(way, d)
                block = self.block(place.origin(way, d), place.core)
                remote(
                    block, block, self.send.at[n], self.recv.at[n], place.sibling()
                ).wait_recv()

            def forward(way=way):
                receive(way)
                if d + 1 < place.chips:
                    self.push(way, d + 1).start()
                self.pass_over(way, d).start()

            def finish(way=way):
                receive(way)
                self.pass_over(way, d).start()

            if onward:
                pl.when(place.behind(way, d) & place.ahead(way) & chosen)(forward)
            if last:
                pl.when(place.behind(way, d) & jnp.logical_not(place.ahead(way)))(finish)

    def arrive(self):
        place = self.place
        for n, (way, d) in enumerate(place.keys):

            def landed(way=way, d=d, n=n):
                block = self.block(place.origin(way, d), 1 - place.core)
                m = self.count + n
                remote(
                    block, block, self.send.at[m], self.recv.at[m], place.sibling()
                ).wait_recv()

            pl.when(place.behind(way, d))(landed)
        block = self.block(place.chip, 1 - place.core)
        m = 2 * self.count
        remote(block, block, self.send.at[m], self.recv.at[m], place.sibling()).wait_recv()

    def close(self):
        place = self.place
        for way, d in place.keys:
            pl.when(place.behind(way, d - 1) & place.ahead(way))(
                lambda way=way, d=d: self.push(way, d).wait_send()
            )
            pl.when(place.behind(way, d))(
                lambda way=way, d=d: self.pass_over(way, d).wait_send()
            )
        self.own_over().wait_send()


def layer_kernel(
    ep_count, tp_count, seq_len, gather_cuts, return_cuts,
    moe_gain_in, routes_in, scores_in, mix_gain_in, pool_scale_in, moe_in, pool_mat,
    shared_gate, shared_up, shared_down, mix_w_in, mix_w_out, mix_in, exp_gate, exp_up, exp_down,
    mixed_out, moe_final,
    *scratch,
):
    scratch = list(scratch)

    def take(count):
        taken, scratch[:] = scratch[:count], scratch[count:]
        return taken

    gathered, sent_back = len(gather_cuts), len(return_cuts)
    tokens, outgoing, received = take(gathered), take(gathered), take(gathered)
    results, returned = take(sent_back), take(sent_back)
    sums, arrived = take(sent_back), take(sent_back)
    (
        pick, share, w_in, w_out, gate_w, up_w, down_w, gate_sum, up_sum,
        s_gate, s_up, s_down, s_gate_sum, s_up_sum, s_hidden, moe_rows, mix_rows, mats, acc, own,
        moe_gain, routes, scores, mix_gain, pool_scale, mixed, moe_out, os,
        ws, xs, xr, ins, inr, outs, outr, as_, ar, bs, br, cs, cr, hs, hr, ss, sr, rs, rr,
    ) = scratch
    place = Place(ep_count, tp_count)
    chips, chip, core = place.chips, place.chip, place.core
    devices = ep_count * tp_count
    flat = place.ep * tp_count + place.tp
    after = (flat + 1) % devices
    after = (after // tp_count, after % tp_count)
    barrier = pltpu.get_barrier_semaphore()

    def greet(device):
        pl.semaphore_signal(barrier, inc=1, device_id=device, device_id_type=MESH)

    rows, width = moe_in.shape
    reach = mix_rows.shape[0] - rows
    stores = (
        (moe_in, moe_rows), (moe_gain_in, moe_gain), (routes_in, routes), (scores_in, scores),
        (shared_gate, s_gate.at[0]), (shared_up, s_up.at[0]), (shared_down, s_down.at[0]),
        (mix_w_in, w_in.at[chip, core]), (mix_w_out, w_out.at[chip, core]),
        (mix_in, mix_rows.at[pl.ds(reach, rows)]), (pool_mat, mats),
        (mix_gain_in, mix_gain), (pool_scale_in, pool_scale),
        (exp_gate.at[0], gate_w), (exp_up.at[0], up_w), (exp_down.at[0], down_w),
    )
    loads = [pltpu.make_async_copy(src, dst, ws.at[n]) for n, (src, dst) in enumerate(stores)]
    for load in loads[:4]:
        load.start()
    near = [place.sibling()] + [(place.partner(i), place.tp) for i in place.turns()]
    for device in near:
        greet(device)
    for way in range(2):
        pl.when(place.ahead(way))(lambda way=way: greet(place.side(way)))
    for load in loads[4:]:
        load.start()
    capacity = outgoing[0].shape[1]
    slots = ep_count * capacity
    block_rows = tp_count * rows
    g_spans, r_spans = spans_of(width, gather_cuts), spans_of(width, return_cuts)
    sent = []

    loads[0].wait()
    loads[1].wait()
    normed = rms_rows(moe_rows[...], moe_gain[...])
    for c, span in enumerate(g_spans):
        tokens[c][pl.ds(chip, 1), pl.ds(core, 1)] = normed[:, span][None, None]
    pl.semaphore_wait(barrier, len(near) + 2 - jnp.where((chip == 0) | (chip == chips - 1), 1, 0))
    gathers = [LineGather(place, tokens[c], xs.at[c], xr.at[c]) for c in range(gathered)]
    for c in range(AHEAD):
        gathers[c].start()

    shared = []
    for n, buf in enumerate((s_gate, s_up, s_down)):
        loads[4 + n].wait()
        copy = remote(buf.at[0], buf.at[1], cs.at[n], cr.at[n], place.sibling())
        copy.start()
        shared.append(copy)

    loads[2].wait()
    loads[3].wait()
    top_count = routes.shape[0]
    lines = CORES * ep_count
    line = lax.broadcasted_iota(jnp.int32, (lines, block_rows), 0)
    column = chip * CORES + jnp.where(line < ep_count, core, 1 - core)
    names = (line % ep_count) * tp_count + column
    score_rows = scores[...].astype(jnp.float32)
    score_sum = jnp.sum(score_rows, axis=0, keepdims=True)
    named = jnp.zeros((lines, block_rows), jnp.float32)
    weight = jnp.zeros((lines, block_rows), jnp.float32)
    for k in range(top_count):
        hit = routes[k : k + 1, :] == names
        named = named + jnp.where(hit, 1.0, 0.0)
        weight = weight + jnp.where(hit, score_rows[k : k + 1, :] / score_sum * ROUTED_SCALE, 0.0)
    ones = named.astype(jnp.bfloat16)
    earlier = []
    for low in range(0, block_rows, 512):
        source = lax.broadcasted_iota(jnp.int32, (block_rows, 512), 0)
        target = lax.broadcasted_iota(jnp.int32, (block_rows, 512), 1) + low
        strict = jnp.where(source < target, 1.0, 0.0).astype(jnp.bfloat16)
        earlier.append(jnp.dot(ones, strict, preferred_element_type=jnp.float32))
    spot = jnp.where(named > 0.5, jnp.concatenate(earlier, axis=1), -1.0).astype(jnp.int32)
    slot = lax.broadcasted_iota(jnp.int32, (capacity, block_rows), 0)
    for j in range(ep_count):
        here = spot[j : j + 1, :] == slot
        pick[j * capacity : (j + 1) * capacity, :] = jnp.where(here, 1.0, 0.0).astype(jnp.bfloat16)
    slot = lax.broadcasted_iota(jnp.int32, (capacity, rows), 0)
    for b in range(chips):
        low = b * CORES * rows
        even, odd = slice(low, low + rows), slice(low + rows, low + 2 * rows)
        spots = jnp.where(core == 0, spot[:, even], spot[:, odd])
        weights = jnp.where(core == 0, weight[:, even], weight[:, odd])
        for j in range(lines):
            weighed = jnp.where(spots[j : j + 1, :] == slot, weights[j : j + 1, :], 0.0)
            share[b, :, j * capacity : (j + 1) * capacity] = weighed.T.astype(jnp.bfloat16)

    def scatter(source, landing, c, send, recv):
        for i in place.turns():
            peer = place.partner(i)
            copy = remote(
                source.at[peer], landing.at[place.ep], send.at[c, i - 1], recv.at[c, i - 1],
                (peer, place.tp),
            )
            copy.start()
            sent.append(copy)
        landing[pl.ds(place.ep, 1)] = source[pl.ds(place.ep, 1)]

    def landing_wait(landing, c, i, send, recv):
        peer = place.partner(i)
        block = landing.at[peer]
        remote(block, block, send.at[c, i - 1], recv.at[c, i - 1], (peer, place.tp)).wait_recv()

    first = LineGather(place, w_in, ins, inr)
    second = LineGather(place, w_out, outs, outr)
    edge = place.edge(chip)
    across = (((1,), (1,)), ((), ()))

    def gate_up(c):
        span = g_spans[c]
        for i in place.turns():
            landing_wait(received[c], c, i, as_, ar)
        block = received[c][...].reshape(slots, span.stop - span.start)
        for acc_ref, weights in ((gate_sum, gate_w), (up_sum, up_w)):
            value = jnp.dot(block, weights[span, :], preferred_element_type=jnp.float32)
            acc_ref[...] = value if c == 0 else acc_ref[...] + value

    def products_of_shared():
        for acc_ref, part in ((s_gate_sum, s_gate), (s_up_sum, s_up)):
            value = 0.0
            for c, span in enumerate(g_spans):
                value = value + lax.dot_general(
                    tokens[c][:, pl.ds(core, 1)].reshape(chips * rows, -1),
                    part[:, :, span].reshape(-1, span.stop - span.start), across,
                    preferred_element_type=jnp.float32,
                )
            acc_ref[...] = value

    lag = 3
    for turn in range(gathered + chips - 2):
        for d in range(1, chips):
            if 0 <= turn - (d - 1) < gathered:
                gathers[turn - (d - 1)].step(d)
            if d == 1 and turn + AHEAD < gathered:
                gathers[turn + AHEAD].start()
        if turn == 0:
            for load in loads[7:13]:
                load.wait()
            for copy in shared:
                copy.wait_recv()
        if turn == max(0, gathered - 1 - AHEAD):

            @pl.when(edge)
            def _():
                first.start(False)
                second.start(False)

        c = turn - (chips - 2)
        if c < 0:
            continue
        gathers[c].arrive()
        cut = g_spans[c].stop - g_spans[c].start
        picked = jnp.dot(
            pick[...], tokens[c][...].reshape(block_rows, cut), preferred_element_type=jnp.float32
        )
        outgoing[c][...] = picked.astype(jnp.bfloat16).reshape(ep_count, capacity, cut)
        scatter(outgoing[c], received[c], c, as_, ar)
        if c == lag:
            for load in loads[13:]:
                load.wait()
        if c >= lag:
            gate_up(c - lag)

    @pl.when(jnp.logical_not(edge))
    def _():
        first.start(False)
        second.start(False)

    first.step(1, last=False, edge=True)
    second.step(1, last=False, edge=True)
    first.own_over().start()
    second.own_over().start()
    halo = remote(
        mix_rows.at[pl.ds(rows, reach)], mix_rows.at[pl.ds(0, reach)], hs, hr, after
    )
    halo.start()

    for c in range(gathered - lag, gathered):
        if c == gathered - 2:
            products_of_shared()
        gate_up(c)
    hidden = (jax.nn.silu(gate_sum[...]) * up_sum[...]).astype(jnp.bfloat16)

    def over(c, i):
        peer = place.partner(i)
        return remote(
            returned[c].at[0, peer], returned[c].at[1, peer], ss.at[c, i], sr.at[c, i],
            place.sibling(),
        )

    def down(c):
        value = jnp.dot(hidden, down_w[:, r_spans[c]], preferred_element_type=jnp.float32)
        results[c][...] = value.astype(jnp.bfloat16).reshape(ep_count, capacity, -1)
        scatter(results[c], returned[c].at[0], c, bs, br)
        over(c, 0).start()

    for c in range(min(LEAD, sent_back)):
        down(c)
    s_hidden[...] = (
        (jax.nn.silu(s_gate_sum[...]) * s_up_sum[...])
        .astype(jnp.bfloat16)
        .reshape(chips, rows, -1)
    )
    first.step(1, last=False, edge=False)

    def routed(c, b):
        span = r_spans[c]
        cut = span.stop - span.start
        value = jnp.dot(
            share[b], returned[c][...].reshape(CORES * slots, cut),
            preferred_element_type=jnp.float32,
        )
        extra = jnp.dot(
            s_hidden[b], s_down[:, :, span].reshape(-1, cut), preferred_element_type=jnp.float32
        )
        acc[:, :cut] = value + extra

    def leaving(way, d):
        return d - 1 if way == 0 else chips - 1 - d

    def reaching(way, d):
        return d - 1 if way == 0 else chips + 1 - d

    def landed(c, way, d, total):
        n = place.key(way, d)
        block = arrived[c].at[reaching(way, d)]
        remote(block, block, rs.at[c, n], rr.at[c, n], place.sibling()).wait_recv()
        total[...] = total[...] + arrived[c][reaching(way, d)].astype(jnp.float32)

    def outward(c, way, d):
        n = place.key(way, d)
        return remote(
            sums[c].at[leaving(way, d)], arrived[c].at[reaching(way, d)], rs.at[c, n],
            rr.at[c, n], place.side(way),
        )

    def from_edge(c, d):
        @pl.when(edge)
        def _():
            up = chip == 0
            pick_way = lambda low, high: jnp.where(up, low, high)
            routed(c, pick_way(place.target(0, d), place.target(1, d)))
            slot = pick_way(leaving(0, d), leaving(1, d))
            cut = r_spans[c].stop - r_spans[c].start
            sums[c][pl.ds(slot, 1)] = acc[:, :cut].astype(jnp.bfloat16)[None]
            n = pick_way(place.key(0, d), place.key(1, d))
            remote(
                sums[c].at[slot], arrived[c].at[pick_way(reaching(0, d), reaching(1, d))],
                rs.at[c, n], rr.at[c, n],
                (place.ep, pick_way(place.target(0, 1), place.target(1, 1)) * CORES + core),
            ).start()

    def from_middle(c, d):
        for way in range(2):

            @pl.when(place.beyond(way, d) & place.ahead(1 - way))
            def _(way=way):
                routed(c, place.target(way, d))
                cut = r_spans[c].stop - r_spans[c].start
                landed(c, way, d + 1, acc.at[:, :cut])
                sums[c][leaving(way, d)] = acc[:, :cut].astype(jnp.bfloat16)
                outward(c, way, d).start()

    def far_middle(c):
        for d in range(chips - 2, 1, -1):
            from_middle(c, d)

    last = sent_back - 1
    for c in range(sent_back):
        if c > 0 and c + LEAD - 1 < sent_back:
            down(c + LEAD - 1)
        for i in place.turns():
            landing_wait(returned[c].at[0], c, i, bs, br)
            over(c, i).start()
        for i in range(ep_count):
            peer = place.partner(i)
            block = returned[c].at[1, peer]
            remote(block, block, ss.at[c, i], sr.at[c, i], place.sibling()).wait_recv()
        for d in range(chips - 1, 0 if c < PROMPT else 1, -1):
            from_edge(c, d)
        if c == 0:
            second.step(1, last=False, edge=False)
        for gather, turn in ((first, 1), (second, 2)):
            if c == min(last, turn):
                for d in range(2, chips):
                    gather.step(d, last=False)
        if c > 0:
            far_middle(c - 1)
        if c > 1:
            from_middle(c - 2, 1)
    far_middle(last)
    for c in range(PROMPT, sent_back):
        from_edge(c, 1)
    for c in range(max(0, last - 1), sent_back):
        from_middle(c, 1)
    for c, span in enumerate(r_spans):
        routed(c, chip)
        own[:, span] = acc[:, : span.stop - span.start]

    for d in range(1, chips):
        first.step(d, onward=False)
    first.arrive()
    halo.wait_recv()
    groups, group_ch = mats.shape[0], mats.shape[1]
    mix_normed = rms_rows(mix_rows[...], mix_gain[...])
    projected = jnp.dot(
        mix_normed, w_in[...].reshape(width, groups * group_ch), preferred_element_type=jnp.float32
    ).astype(jnp.bfloat16)
    first_row = flat * rows
    keep = jnp.where(first_row % seq_len == 0, 0.0, 1.0)
    projected = projected.astype(jnp.float32)
    extended = jnp.concatenate([projected[:reach] * keep, projected[reach:]], axis=0)
    position = (first_row + lax.broadcasted_iota(jnp.int32, (rows, group_ch), 0)) % seq_len
    pooled_parts = []
    for group in range(groups):
        channels = slice(group * group_ch, (group + 1) * group_ch)
        running = extended[:, channels]
        for level in range(group + 1):
            running = running + pltpu.roll(running, 2**level, 0)
        counts = jnp.minimum(position + 1, 2 ** (group + 1)).astype(jnp.float32)
        pooled = (running[reach:] / counts - extended[reach:, channels]).astype(jnp.bfloat16)
        grouped = jnp.dot(pooled, mats[group], preferred_element_type=jnp.float32)
        pooled_parts.append((grouped * pool_scale[:, channels]).astype(jnp.bfloat16))
    pool_out = jnp.concatenate(pooled_parts, axis=1)
    for d in range(1, chips):
        second.step(d, onward=False)
    second.arrive()
    span = w_out.shape[3]
    for column in range(tp_count):
        mixed[:, column * span : (column + 1) * span] = jnp.dot(
            pool_out, w_out[column // CORES, column % CORES], preferred_element_type=jnp.float32
        ).astype(jnp.bfloat16)

    outs = [pltpu.make_async_copy(mixed, mixed_out, os.at[sent_back])]
    outs[0].start()
    for c, span in enumerate(r_spans):
        for way in range(2):

            def join(way=way):
                landed(c, way, 1, own.at[:, span])

            pl.when(place.behind(way, 1))(join)
        moe_out[:, span] = own[:, span].astype(jnp.bfloat16)
        out = pltpu.make_async_copy(moe_out.at[:, span], moe_final.at[:, span], os.at[c])
        out.start()
        outs.append(out)

    halo.wait_send()
    for out in outs:
        out.wait()
    for copy in sent + shared:
        copy.wait_send()
    for c in range(sent_back):
        for i in range(ep_count):
            over(c, i).wait_send()
        for way, d in place.keys:
            pl.when(place.beyond(way, d))(
                lambda way=way, d=d: outward(c, way, d).wait_send()
            )
    for gather in gathers + [first, second]:
        gather.close()


def settle_kernel(mixed, moe, mixed_out, moe_out, held, arrive, leave):
    rows = mixed.shape[0] // CHUNKS
    inward, outward = [], []
    for n, (src, dst) in enumerate(((mixed, mixed_out), (moe, moe_out))):
        for k in range(CHUNKS):
            span = pl.ds(k * rows, rows)
            block = held.at[n, span]
            inward.append(pltpu.make_async_copy(src.at[span], block, arrive.at[n, k]))
            outward.append(pltpu.make_async_copy(block, dst.at[span], leave.at[n, k]))
    for copy in inward:
        copy.start()
    for n, copy in enumerate(inward):
        copy.wait()
        outward[n].start()
    for copy in outward:
        copy.wait()


def shards(
    mix_in, mix_gain, mix_w_in, pool_mat, pool_scale, mix_w_out, moe_in, moe_gain, routes,
    route_score, exp_gate, exp_up, exp_down, shared_gate, shared_up, shared_down,
):
    ep_count, tp_count = lax.axis_size("ep"), lax.axis_size("tp")
    rows, width = moe_in.shape
    block_rows, top_count = routes.shape
    capacity = 2 * block_rows * top_count // (ep_count * tp_count)
    slots = ep_count * capacity
    dma = lambda *shape: pltpu.SemaphoreType.DMA(shape)
    bf16, f32 = jnp.bfloat16, jnp.float32

    chips = tp_count // CORES
    messages = 2 * (chips - 1)
    hidden, s_hidden = exp_gate.shape[2], shared_gate.shape[0]
    reach = 2 ** pool_mat.shape[0]
    seq_len = mix_in.shape[0] * ep_count * tp_count // SEQS_MIX
    buffer = lambda *shape: pltpu.VMEM(shape, bf16)
    g_cuts = [s.stop - s.start for s in spans_of(width, GATHER_CUTS)]
    r_cuts = [s.stop - s.start for s in spans_of(width, RETURN_CUTS)]
    gathered, sent_back = len(g_cuts), len(r_cuts)
    scratch = (
        [buffer(chips, CORES, rows, cut) for cut in g_cuts]
        + [buffer(ep_count, capacity, cut) for cut in g_cuts] * 2
        + [buffer(ep_count, capacity, cut) for cut in r_cuts]
        + [buffer(CORES, ep_count, capacity, cut) for cut in r_cuts]
        + [buffer(chips - 1, rows, cut) for cut in r_cuts]
        + [buffer(chips + 1, rows, cut) for cut in r_cuts]
        + [
            buffer(slots, block_rows),
            buffer(chips, rows, CORES * slots),
            buffer(chips, CORES, *mix_w_in.shape),
            buffer(chips, CORES, *mix_w_out.shape),
            buffer(width, hidden),
            buffer(width, hidden),
            buffer(hidden, width),
            pltpu.VMEM((slots, hidden), f32),
            pltpu.VMEM((slots, hidden), f32),
            buffer(CORES, *shared_gate.shape),
            buffer(CORES, *shared_up.shape),
            buffer(CORES, *shared_down.shape),
            pltpu.VMEM((chips * rows, CORES * s_hidden), f32),
            pltpu.VMEM((chips * rows, CORES * s_hidden), f32),
            buffer(chips, rows, CORES * s_hidden),
            buffer(*moe_in.shape),
            buffer(mix_in.shape[0] + reach, width),
            buffer(*pool_mat.shape),
            pltpu.VMEM((rows, max(r_cuts)), f32),
            pltpu.VMEM((rows, width), f32),
            pltpu.VMEM((1, width), f32),
            pltpu.VMEM((top_count, block_rows), routes.dtype),
            buffer(top_count, block_rows),
            pltpu.VMEM((1, width), f32),
            pltpu.VMEM((1, pool_scale.shape[0]), f32),
            buffer(*mix_in.shape),
            buffer(*moe_in.shape),
            dma(1 + sent_back),
            dma(16),
            dma(gathered, 2 * messages + 1),
            dma(gathered, 2 * messages + 1),
        ]
        + [dma(2 * messages + 1)] * 4
        + [dma(gathered, ep_count - 1)] * 2
        + [dma(sent_back, ep_count - 1)] * 2
        + [dma(3), dma(3)]
        + [pltpu.SemaphoreType.DMA, pltpu.SemaphoreType.DMA]
        + [dma(sent_back, ep_count)] * 2
        + [dma(sent_back, messages)] * 2
    )
    mixed, moe_out = pl.pallas_call(
        functools.partial(layer_kernel, ep_count, tp_count, seq_len, GATHER_CUTS, RETURN_CUTS),
        out_shape=[
            jax.ShapeDtypeStruct(mix_in.shape, bf16),
            jax.ShapeDtypeStruct(moe_in.shape, bf16),
        ],
        in_specs=[pl.BlockSpec(memory_space=pltpu.HBM)] * 16,
        out_specs=[pl.BlockSpec(memory_space=pltpu.HBM)] * 2,
        scratch_shapes=scratch,
        compiler_params=pltpu.CompilerParams(
            collective_id=0, has_side_effects=True, vmem_limit_bytes=VMEM_BYTES
        ),
    )(
        moe_gain[None, :], routes.T, route_score.T, mix_gain[None, :], pool_scale[None, :],
        moe_in, pool_mat, shared_gate, shared_up, shared_down, mix_w_in, mix_w_out, mix_in,
        exp_gate, exp_up, exp_down,
    )
    return pl.pallas_call(
        settle_kernel,
        out_shape=[
            jax.ShapeDtypeStruct(mix_in.shape, bf16),
            jax.ShapeDtypeStruct(moe_in.shape, bf16),
        ],
        in_specs=[pl.BlockSpec(memory_space=pltpu.HBM)] * 2,
        out_specs=[pl.BlockSpec(memory_space=pltpu.HBM)] * 2,
        scratch_shapes=[buffer(2, *mix_in.shape), dma(2, CHUNKS), dma(2, CHUNKS)],
        compiler_params=pltpu.CompilerParams(vmem_limit_bytes=VMEM_BYTES),
    )(mixed, moe_out)


def solution(mesh):
    return jax.shard_map(
        shards,
        mesh=mesh,
        in_specs=(
            P(("ep", "tp"), None),
            P(),
            P("tp", None),
            P(),
            P(),
            P(None, "tp"),
            P(("ep", "tp"), None),
            P(),
            P("ep", None),
            P("ep", None),
            P(("ep", "tp"), None, None),
            P(("ep", "tp"), None, None),
            P(("ep", "tp"), None, None),
            P("tp", None),
            P("tp", None),
            P("tp", None),
        ),
        out_specs=(P(("ep", "tp"), None), P(("ep", "tp"), None)),
        check_vma=False,
    )
```
